32 devices in a mesh: sp: 8 (over z, x), tp: 4 (over y, core).
Axes of the slice: x: 2, y: 2, z: 4, core: 2. Of those that a mesh axis runs over, the one named last changes fastest.
Arguments:
- tokens: bfloat16 [4096, 4096], P(('sp', 'tp')), may hold values from -6 to 6
- lock_projector: bfloat16 [4096, 1024], P(None, 'tp'), may hold values from -0.01171875 to 0.01171875
- value_weight: bfloat16 [4096, 2048], P(None, 'tp'), may hold values from -0.0234375 to 0.0234375
- decay_weight: bfloat16 [4096, 1024], P(None, 'tp'), may hold values from -0.09375 to 0.09375
- decay_offset: float32 [1024], P('tp'), may hold values from -3.5 to 0
- fresh_question: bfloat16 [16, 64], P('tp'), may hold values from -6 to 6
Outputs:
- state_cache: bfloat16 [16, 64, 128], P('tp', 'sp')
- first_read: bfloat16 [16, 128], P('tp')
The draws below stay inside these ranges and needn't reach their ends.
All inputs are finite; a program needn't handle non-finite values.
Results may differ from the reference program's by a relative error of at most 0.0034.
Values may be sent and summed in bfloat16 or wider, within the bound.
No kernel may reach another device: no remote copies, remote signals or barrier semaphores. Data moves between devices by JAX's collectives and lax.ppermute only.
A program may use at most 64 MiB of HBM per device.

```python
import math
import jax
import jax.numpy as jnp
from jax import lax

D = 4096
H = 16
CUE_WIDTH = 64
DV = 128
PROMPT_SPAN = 4096


def block_levels(key, extent, pieces, low, high):
    factor_of = 1.0
    for position, blocks in pieces:
        heights = jax.random.uniform(jax.random.fold_in(jax.random.fold_in(key, 6), position), (blocks,), jnp.float32, low / len(pieces), high / len(pieces))
        factor_of = factor_of * jnp.repeat(jnp.exp(heights), extent[position] // blocks).reshape((-1,) + (1,) * (len(extent) - 1 - position))
    return factor_of


def noise(key, dims, scale, limit, shards=(), dtype=jnp.bfloat16):
    entries = scale * jax.random.normal(key, dims, jnp.float32)
    if shards:
        entries = entries * block_levels(key, dims, shards, -0.22, 0.18)
    return jnp.clip(entries, -limit, limit).astype(dtype)


def setup_inputs(seed: int = 0) -> dict:
    key_of = jax.random.split(jax.random.key(seed), 7)
    tokens = noise(key_of[0], (PROMPT_SPAN, D), 1.0, 6.0, ((0, 32),))
    lock_projector = noise(key_of[1], (D, H * CUE_WIDTH), (D * CUE_WIDTH) ** -0.5, 0.01171875, ((1, 4),))
    value_weight = noise(key_of[2], (D, H * DV), (D * 16) ** -0.5, 0.0234375, ((1, 4),))
    decay_weight = noise(key_of[3], (D, H * CUE_WIDTH), D ** -0.5, 0.09375, ((1, 4),))
    decay_offset = jnp.clip(-3.5 + 3.5 * jax.random.uniform(key_of[4], (H * CUE_WIDTH,), jnp.float32) ** block_levels(key_of[4], (H * CUE_WIDTH,), ((0, 4),), -0.2, 0.2), -3.5, 0.0)
    fresh_question = noise(key_of[5], (H, CUE_WIDTH), 1.0, 6.0, ((0, 4),))
    return dict(tokens=tokens, lock_projector=lock_projector, value_weight=value_weight, decay_weight=decay_weight, decay_offset=decay_offset, fresh_question=fresh_question)


decay_tau = 16.0

def reference(tokens, lock_projector, value_weight, decay_weight, decay_offset, fresh_question):
    lock_vectors = jnp.dot(tokens, lock_projector, preferred_element_type=jnp.float32).astype(jnp.bfloat16)
    value_rows = jnp.dot(tokens, value_weight, preferred_element_type=jnp.float32).astype(jnp.bfloat16)
    decay_pre = jnp.dot(tokens, decay_weight, preferred_element_type=jnp.float32)
    log_decay = jax.nn.log_sigmoid(decay_pre + decay_offset[None, :] + math.log(PROMPT_SPAN)) / decay_tau
    totals = lax.optimization_barrier(jnp.sum(log_decay, axis=0))
    after = totals[None, :] - jnp.cumsum(log_decay, axis=0)
    weighted = (lock_vectors.astype(jnp.float32) * jnp.exp(after)).astype(jnp.bfloat16)
    lookup_probes = weighted.astype(jnp.float32).reshape(PROMPT_SPAN, H, CUE_WIDTH)
    stored_contents = value_rows.astype(jnp.float32).reshape(PROMPT_SPAN, H, DV)
    recall_grid = jnp.einsum('nyl,nyp->ylp', lookup_probes, stored_contents)
    attended_blend = CUE_WIDTH ** (-0.5) * jnp.einsum('qw,qwi->qi', fresh_question.astype(jnp.float32), recall_grid, precision=lax.Precision.HIGHEST)
    first_read = attended_blend * lax.rsqrt(lax.optimization_barrier(jnp.mean(attended_blend * attended_blend, axis=-1, keepdims=True)) + 1.0)
    return (recall_grid.astype(jnp.bfloat16), first_read.astype(jnp.bfloat16))
```

```python
import functools
import math

import jax
import jax.numpy as jnp
from jax import lax
from jax.experimental import pallas as pl
from jax.experimental.pallas import tpu as pltpu
from jax.sharding import PartitionSpec as P


CUE_WIDTH = 64
DV = 128
DECAY_TAU = 16.0
LATE_PARTS = 4
VMEM_LIMIT = 24 * 1024 * 1024


F32 = jnp.float32
BF16 = jnp.bfloat16
EXACT = lax.Precision.HIGHEST


def swap(count, bit):
    return [(i, i ^ bit) for i in range(count)]


def project(x, wk, wv, wd, offset, log_length):
    keys = jnp.dot(x, wk[...], preferred_element_type=F32).astype(BF16)
    values = jnp.dot(x, wv[...], preferred_element_type=F32).astype(BF16)
    pre = jnp.dot(x, wd[...], preferred_element_type=F32)
    z = pre + offset + log_length
    log_decay = (jnp.minimum(z, 0.0) - jnp.log1p(jnp.exp(-jnp.abs(z)))) / DECAY_TAU
    return keys, values, log_decay


def later_within(log_decay, blocks):
    rows = log_decay.shape[0]
    size = rows // blocks
    i = lax.broadcasted_iota(jnp.int32, (rows, rows), 0)
    j = lax.broadcasted_iota(jnp.int32, (rows, rows), 1)
    mask = j > i
    for b in range(1, blocks):
        mask = mask & ((i >= b * size) == (j >= b * size))
    return jnp.dot(mask.astype(F32), log_decay, precision=EXACT, preferred_element_type=F32)


def weigh(keys, after):
    exact = keys.astype(F32) * jnp.exp(after)
    high = exact.astype(BF16)
    return high, (exact - high.astype(F32)).astype(BF16)


def outer(values, weighted):
    high, low = weighted
    heads = high.shape[1] // CUE_WIDTH
    group = min(2, heads)
    cols = group * CUE_WIDTH
    parts = []
    for g in range(heads // group):
        w = jnp.concatenate([p[:, g * cols : (g + 1) * cols] for p in (high, low)], axis=1)
        v = values[:, g * group * DV : (g + 1) * group * DV]
        full = lax.dot_general(v, w, (((0,), (0,)), ((), ())), preferred_element_type=F32)
        full = full[:, :cols] + full[:, cols:]
        kept = full[:DV]
        if group == 2:
            lane = lax.broadcasted_iota(jnp.int32, kept.shape, 1)
            kept = jnp.where(lane < CUE_WIDTH, kept, full[DV:])
        parts.append(kept)
    return parts[0] if len(parts) == 1 else jnp.concatenate(parts, axis=1)


def payload_sds(heads):
    pad = -(3 + 3 * heads) % 16
    width = max(heads * CUE_WIDTH, DV)
    return jax.ShapeDtypeStruct((DV + 3 + 3 * heads + pad, width), BF16)


def split(exact):
    parts, rest = [], exact
    for _ in range(3):
        parts.append(rest.astype(BF16).astype(F32))
        rest = rest - parts[-1]
    return parts


def widen(x, width):
    extra = width - x.shape[1]
    return jnp.concatenate([x, jnp.zeros((x.shape[0], extra), x.dtype)], axis=1) if extra else x


def pack(out, state, total, heard=None):
    width = out.shape[1]
    rows = [widen(p, width) for p in split(total)]
    if heard is not None:
        for part in split(heard):
            part = widen(part, width)
            rows += [part[h : h + 1] for h in range(part.shape[0])]
    row = lax.broadcasted_iota(jnp.int32, (out.shape[0] - DV, width), 0)
    tail = jnp.zeros(row.shape, F32)
    for n, value in enumerate(rows):
        tail = jnp.where(row == n, value, tail)
    out[:DV, :] = widen(state.astype(BF16), width)
    out[DV:, :] = tail.astype(BF16)


def unpack(ref, key_cols):
    tail = ref[DV:, :].astype(F32)
    total = tail[0:1] + tail[1:2] + tail[2:3]
    return ref[:DV, :key_cols].astype(F32), total[:, :key_cols], tail


def heard_of(tail, heads):
    parts = [tail[3 + n * heads : 3 + (n + 1) * heads, :DV] for n in range(3)]
    return parts[0] + parts[1] + parts[2]


def asking(question, rows):
    row = lax.broadcasted_iota(jnp.int32, (rows, question.shape[1]), 0)
    lane = lax.broadcasted_iota(jnp.int32, (rows, question.shape[1]), 1)
    asked = question[...].astype(F32) * CUE_WIDTH ** (-0.5)
    return jnp.where(lax.div(lane, CUE_WIDTH) == row, asked, 0.0)


def against(left, state):
    return lax.dot_general(
        left, state, (((1,), (1,)), ((), ())), precision=EXACT, preferred_element_type=F32
    )


def near_kernel(x0, x1, wk, wv, wd, off, s_out, l_out, *, log_length):
    core = lax.rem(lax.axis_index("tp"), 2)
    rows = x0.shape[0]
    x = jnp.concatenate([x0[...], x1[...]], axis=0)
    keys, values, log_decay = project(x, wk, wv, wd, off[...], log_length)
    after = later_within(log_decay, 2)
    own = after[0:1] + log_decay[0:1]
    sib = after[rows : rows + 1] + log_decay[rows : rows + 1]
    own_tail = jnp.where(core == 0, sib, 0.0)
    sib_tail = jnp.where(core == 0, 0.0, own)
    row = lax.broadcasted_iota(jnp.int32, after.shape, 0)
    after = after + jnp.where(row < rows, own_tail, sib_tail)
    s_out[...] = outer(values, weigh(keys, after))
    l_out[...] = own + sib


def early_kernel(xa, xb, wk, wv, wd, off, s_a, s_b, l_a, l_b, *, log_length):
    rows = xa.shape[0]
    x = jnp.concatenate([xa[...], xb[...]], axis=0)
    keys, values, log_decay = project(x, wk, wv, wd, off[...], log_length)
    after = later_within(log_decay, 2)
    weighted = weigh(keys, after)
    s_a[...] = outer(values[:rows], [w[:rows] for w in weighted])
    s_b[...] = outer(values[rows:], [w[rows:] for w in weighted])
    l_a[...] = after[0:1] + log_decay[0:1]
    l_b[...] = after[rows : rows + 1] + log_decay[rows : rows + 1]


def late_kernel(xa, xb, wk, wv, wd, off, *refs, log_length, blocks, here, parts):
    states = refs[: len(blocks)]
    totals = refs[len(blocks) : 2 * len(blocks)]
    out = refs[2 * len(blocks)]
    place = lax.axis_index("tp")
    core = lax.rem(place, 2)
    chip = lax.div(place, 2)
    rows = xa.shape[0]

    def position(block):
        if block is None:
            return chip * (2 * parts)
        bit, part, same = block
        parity = core if same else 1 - core
        return lax.bitwise_xor(chip, bit) * (2 * parts) + parity * parts + part

    x = jnp.concatenate([xa[...], xb[...]], axis=0)
    keys, values, log_decay = project(x, wk, wv, wd, off[...], log_length)
    after = later_within(log_decay, 2)
    own = [
        after[0:1] + log_decay[0:1],
        after[rows : rows + 1] + log_decay[rows : rows + 1],
    ]
    every = [(position(b), totals[n][...]) for n, b in enumerate(blocks)]
    mine = [position(here + (True,)), position(here + (False,))]
    every += list(zip(mine, own))

    def later_of(pos):
        acc = jnp.zeros_like(own[0])
        for p, t in every:
            acc = acc + jnp.where(p > pos, t, 0.0)
        return acc

    row = lax.broadcasted_iota(jnp.int32, after.shape, 0)
    after = after + jnp.where(row < rows, later_of(mine[0]), later_of(mine[1]))
    state = outer(values, weigh(keys, after))
    total = own[0] + own[1]
    for n in range(len(blocks)):
        pos, t = every[n]
        state = state + states[n][...] * jnp.exp(later_of(pos))
        total = total + t
    pack(out, state, total)


def merge_kernel(question, *refs, bits):
    count = 2 ** len(bits)
    out, exact = refs[count:]
    key_cols = question.shape[1]
    parts = [unpack(ref, key_cols)[:2] for ref in refs[:count]]
    for n, bit in enumerate(bits):
        turned = lax.bitwise_and(lax.axis_index("sp"), bit) != 0
        parts = [
            tuple(jnp.where(turned, x, y) for x, y in zip(parts[k ^ (1 << n)], parts[k]))
            for k in range(count)
        ]
    state, total = parts[0]
    for s, t in parts[1:]:
        state = state * jnp.exp(t) + s
        total = total + t
    exact[...] = state
    heads = key_cols // CUE_WIDTH
    pack(out, state, total, against(asking(question, 8), state)[:heads])


def final_kernel(question, mine, other, exact, cache, read, *, bit):
    heads, kept, _ = cache.shape
    key_cols = question.shape[1]
    earlier = lax.bitwise_and(lax.axis_index("sp"), bit) == 0
    s_m, l_m, tail_m = unpack(mine, key_cols)
    s_o, l_o, tail_o = unpack(other, key_cols)
    fading = jnp.exp(jnp.where(earlier, l_o, l_m))
    first = jnp.where(earlier, s_m, s_o) * fading
    state = jnp.where(earlier, exact[...] * fading + s_o, first + exact[...])
    rows = heads * kept
    rows += -rows % 8
    row = lax.broadcasted_iota(jnp.int32, (rows, key_cols), 0)
    lane = lax.broadcasted_iota(jnp.int32, (rows, key_cols), 1)
    start = lax.axis_index("sp") * kept
    column = lax.div(row, kept) * CUE_WIDTH + start + lax.rem(row, kept)
    chosen = ((row < heads * kept) & (lane == column)).astype(F32)
    result = against(chosen, state)
    for h in range(heads):
        cache[h] = result[h * kept : (h + 1) * kept].astype(BF16)
    heard = against(asking(question, 8), first)[:heads]
    heard = heard + heard_of(jnp.where(earlier, tail_o, tail_m), heads)
    mean = jnp.mean(heard * heard, axis=-1, keepdims=True)
    read[...] = (heard * lax.rsqrt(mean + 1.0)).astype(BF16)


VM = pl.BlockSpec(memory_space=pltpu.VMEM)


def call(kernel, out_shape, in_specs, scratch=(), flops=0):
    return pl.pallas_call(
        kernel,
        out_shape=out_shape,
        in_specs=in_specs,
        out_specs=jax.tree.map(lambda _: VM, out_shape),
        scratch_shapes=list(scratch),
        cost_estimate=pl.CostEstimate(flops=flops, bytes_accessed=0, transcendentals=0),
        compiler_params=pltpu.CompilerParams(vmem_limit_bytes=VMEM_LIMIT),
    )


def whole(sp, tp, tokens, wk, wv, wd, decay_offset, fresh_question):
    rows, width = tokens.shape
    key_cols, value_cols = wk.shape[1], wv.shape[1]
    heads = key_cols // CUE_WIDTH
    cols = 2 * key_cols + value_cols
    log_length = math.log(rows * tp * sp)
    offset = decay_offset.reshape(1, key_cols)
    question = fresh_question.reshape(1, key_cols)
    sds = jax.ShapeDtypeStruct
    state_sds = sds((DV, key_cols), F32)
    total_sds = sds((1, key_cols), F32)

    late = rows // LATE_PARTS
    cuts = [(0, rows - late), (rows - late, rows)]
    far = {}
    for bit in range(1, tp // 2):
        for part, (lo, hi) in enumerate(cuts):
            far[bit, part] = lax.ppermute(tokens[lo:hi], "tp", swap(tp, 2 * bit))
    sibling = lax.ppermute(tokens, "tp", swap(tp, 1))

    s_near, l_near = call(
        functools.partial(near_kernel, log_length=log_length),
        (state_sds, total_sds),
        [VM] * 6,
        flops=4 * rows * width * cols,
    )(tokens, sibling, wk, wv, wd, offset)

    blocks, states, totals = [None], [s_near], [l_near]
    payload = None
    order = list(far)
    for n, (bit, part) in enumerate(order):
        a = far[bit, part]
        b = lax.ppermute(a, "tp", swap(tp, 1))
        flops = 4 * a.shape[0] * width * cols
        if n < len(order) - 1:
            s_a, s_b, l_a, l_b = call(
                functools.partial(early_kernel, log_length=log_length),
                (state_sds, state_sds, total_sds, total_sds),
                [VM] * 6,
                flops=flops,
            )(a, b, wk, wv, wd, offset)
            blocks += [(bit, part, True), (bit, part, False)]
            states += [s_a, s_b]
            totals += [l_a, l_b]
        else:
            payload = call(
                functools.partial(
                    late_kernel,
                    log_length=log_length,
                    blocks=tuple(blocks),
                    here=(bit, part),
                    parts=len(cuts),
                ),
                payload_sds(heads),
                [VM] * (6 + 2 * len(blocks)),
                flops=flops,
            )(a, b, wk, wv, wd, offset, *states, *totals)

    bits = [1 << n for n in range(sp.bit_length() - 1)]
    while len(bits) > 1:
        take = 2 if len(bits) > 2 else 1
        group, bits = bits[:take], bits[take:]
        others = [
            lax.ppermute(payload, "sp", swap(sp, sum(b for n, b in enumerate(group) if k >> n & 1)))
            for k in range(1, 2**take)
        ]
        payload, exact = call(
            functools.partial(merge_kernel, bits=tuple(group)),
            (payload_sds(heads), state_sds),
            [VM] * (2 + len(others)),
        )(question, payload, *others)
    other = lax.ppermute(payload, "sp", swap(sp, bits[0]))
    return call(
        functools.partial(final_kernel, bit=bits[0]),
        (sds((heads, CUE_WIDTH // sp, DV), BF16), sds((heads, DV), BF16)),
        [VM] * 4,
    )(question, payload, other, exact)


def solution(mesh):
    sp, tp = mesh.shape["sp"], mesh.shape["tp"]
    in_specs = (
        P(("sp", "tp"), None),
        P(None, "tp"),
        P(None, "tp"),
        P(None, "tp"),
        P("tp"),
        P("tp", None),
    )
    out_specs = (P("tp", "sp", None), P("tp", None))
    return jax.shard_map(
        functools.partial(whole, sp, tp),
        mesh=mesh,
        in_specs=in_specs,
        out_specs=out_specs,
        check_vma=False,
    )
```

```python
import functools
import math

import jax
import jax.numpy as jnp
from jax import lax
from jax.experimental import pallas as pl
from jax.experimental.pallas import tpu as pltpu
from jax.sharding import PartitionSpec as P


CUE_WIDTH = 64
DV = 128
DECAY_TAU = 16.0
ROW_PARTS = (1, 5, 2)
VMEM_LIMIT = 24 * 1024 * 1024


F32 = jnp.float32
BF16 = jnp.bfloat16
EXACT = lax.Precision.HIGHEST


def swap(count, bit):
    return [(i, i ^ bit) for i in range(count)]


def project(x, wk, wv, wd, offset, log_length):
    keys = jnp.dot(x, wk[...], preferred_element_type=F32).astype(BF16)
    values = jnp.dot(x, wv[...], preferred_element_type=F32).astype(BF16)
    pre = jnp.dot(x, wd[...], preferred_element_type=F32)
    z = pre + offset + log_length
    log_decay = (jnp.minimum(z, 0.0) - jnp.log1p(jnp.exp(-jnp.abs(z)))) / DECAY_TAU
    return keys, values, log_decay


def later_within(log_decay, sizes):
    rows = log_decay.shape[0]
    i = lax.broadcasted_iota(jnp.int32, (rows, rows), 0)
    j = lax.broadcasted_iota(jnp.int32, (rows, rows), 1)
    mask = j > i
    edge = 0
    for size in sizes[:-1]:
        edge += size
        mask = mask & ((i >= edge) == (j >= edge))
    return jnp.dot(mask.astype(F32), log_decay, precision=EXACT, preferred_element_type=F32)


def weigh(keys, after):
    exact = keys.astype(F32) * jnp.exp(after)
    high = exact.astype(BF16)
    return high, (exact - high.astype(F32)).astype(BF16)


def outer(values, weighted):
    high, low = weighted
    heads = high.shape[1] // CUE_WIDTH
    group = min(2, heads)
    cols = group * CUE_WIDTH
    parts = []
    for g in range(heads // group):
        w = jnp.concatenate([p[:, g * cols : (g + 1) * cols] for p in (high, low)], axis=1)
        v = values[:, g * group * DV : (g + 1) * group * DV]
        full = lax.dot_general(v, w, (((0,), (0,)), ((), ())), preferred_element_type=F32)
        full = full[:, :cols] + full[:, cols:]
        kept = full[:DV]
        if group == 2:
            lane = lax.broadcasted_iota(jnp.int32, kept.shape, 1)
            kept = jnp.where(lane < CUE_WIDTH, kept, full[DV:])
        parts.append(kept)
    return parts[0] if len(parts) == 1 else jnp.concatenate(parts, axis=1)


def payload_sds(heads):
    pad = -(3 + 3 * heads) % 16
    width = max(heads * CUE_WIDTH, DV)
    return jax.ShapeDtypeStruct((DV + 3 + 3 * heads + pad, width), BF16)


def split(exact):
    parts, rest = [], exact
    for _ in range(3):
        parts.append(rest.astype(BF16).astype(F32))
        rest = rest - parts[-1]
    return parts


def widen(x, width):
    extra = width - x.shape[1]
    return jnp.concatenate([x, jnp.zeros((x.shape[0], extra), x.dtype)], axis=1) if extra else x


def pack(out, state, total, heard=None):
    width = out.shape[1]
    rows = [widen(p, width) for p in split(total)]
    if heard is not None:
        for part in split(heard):
            part = widen(part, width)
            rows += [part[h : h + 1] for h in range(part.shape[0])]
    row = lax.broadcasted_iota(jnp.int32, (out.shape[0] - DV, width), 0)
    tail = jnp.zeros(row.shape, F32)
    for n, value in enumerate(rows):
        tail = jnp.where(row == n, value, tail)
    out[:DV, :] = widen(state.astype(BF16), width)
    out[DV:, :] = tail.astype(BF16)


def unpack(ref, key_cols):
    tail = ref[DV:, :].astype(F32)
    total = tail[0:1] + tail[1:2] + tail[2:3]
    return ref[:DV, :key_cols].astype(F32), total[:, :key_cols], tail


def heard_of(tail, heads):
    parts = [tail[3 + n * heads : 3 + (n + 1) * heads, :DV] for n in range(3)]
    return parts[0] + parts[1] + parts[2]


def asking(question, rows):
    row = lax.broadcasted_iota(jnp.int32, (rows, question.shape[1]), 0)
    lane = lax.broadcasted_iota(jnp.int32, (rows, question.shape[1]), 1)
    asked = question[...].astype(F32) * CUE_WIDTH ** (-0.5)
    return jnp.where(lax.div(lane, CUE_WIDTH) == row, asked, 0.0)


def against(left, state):
    return lax.dot_general(
        left, state, (((1,), (1,)), ((), ())), precision=EXACT, preferred_element_type=F32
    )


def near_kernel(x0, x1, wk, wv, wd, off, s_out, l_out, *, log_length):
    core = lax.rem(lax.axis_index("tp"), 2)
    rows = x0.shape[0]
    x = jnp.concatenate([x0[...], x1[...]], axis=0)
    keys, values, log_decay = project(x, wk, wv, wd, off[...], log_length)
    after = later_within(log_decay, [rows, rows])
    own = after[0:1] + log_decay[0:1]
    sib = after[rows : rows + 1] + log_decay[rows : rows + 1]
    own_tail = jnp.where(core == 0, sib, 0.0)
    sib_tail = jnp.where(core == 0, 0.0, own)
    row = lax.broadcasted_iota(jnp.int32, after.shape, 0)
    after = after + jnp.where(row < rows, own_tail, sib_tail)
    s_out[...] = outer(values, weigh(keys, after))
    l_out[...] = own + sib


def early_kernel(*refs, log_length, blocks):
    wk, wv, wd, off = refs[blocks : blocks + 4]
    outs = refs[blocks + 4 :]
    sizes = [ref.shape[0] for ref in refs[:blocks]]
    x = jnp.concatenate([ref[...] for ref in refs[:blocks]], axis=0)
    keys, values, log_decay = project(x, wk, wv, wd, off[...], log_length)
    after = later_within(log_decay, sizes)
    weighted = weigh(keys, after)
    lo = 0
    for n, size in enumerate(sizes):
        hi = lo + size
        outs[n][...] = outer(values[lo:hi], [w[lo:hi] for w in weighted])
        outs[blocks + n][...] = after[lo : lo + 1] + log_decay[lo : lo + 1]
        lo = hi


def late_kernel(xa, xb, wk, wv, wd, off, *refs, log_length, blocks, here, parts):
    states = refs[: len(blocks)]
    totals = refs[len(blocks) : 2 * len(blocks)]
    out = refs[2 * len(blocks)]
    place = lax.axis_index("tp")
    core = lax.rem(place, 2)
    chip = lax.div(place, 2)
    rows = xa.shape[0]

    def position(block):
        if block is None:
            return chip * (2 * parts)
        bit, part, same = block
        parity = core if same else 1 - core
        return lax.bitwise_xor(chip, bit) * (2 * parts) + parity * parts + part

    x = jnp.concatenate([xa[...], xb[...]], axis=0)
    keys, values, log_decay = project(x, wk, wv, wd, off[...], log_length)
    after = later_within(log_decay, [rows, rows])
    own = [
        after[0:1] + log_decay[0:1],
        after[rows : rows + 1] + log_decay[rows : rows + 1],
    ]
    every = [(position(b), totals[n][...]) for n, b in enumerate(blocks)]
    mine = [position(here + (True,)), position(here + (False,))]
    every += list(zip(mine, own))

    def later_of(pos):
        acc = jnp.zeros_like(own[0])
        for p, t in every:
            acc = acc + jnp.where(p > pos, t, 0.0)
        return acc

    row = lax.broadcasted_iota(jnp.int32, after.shape, 0)
    after = after + jnp.where(row < rows, later_of(mine[0]), later_of(mine[1]))
    state = outer(values, weigh(keys, after))
    total = own[0] + own[1]
    for n in range(len(blocks)):
        pos, t = every[n]
        state = state + states[n][...] * jnp.exp(later_of(pos))
        total = total + t
    pack(out, state, total)


def merge_kernel(question, *refs, bits):
    count = 2 ** len(bits)
    out, exact = refs[count:]
    key_cols = question.shape[1]
    parts = [unpack(ref, key_cols)[:2] for ref in refs[:count]]
    for n, bit in enumerate(bits):
        turned = lax.bitwise_and(lax.axis_index("sp"), bit) != 0
        parts = [
            tuple(jnp.where(turned, x, y) for x, y in zip(parts[k ^ (1 << n)], parts[k]))
            for k in range(count)
        ]
    state, total = parts[0]
    for s, t in parts[1:]:
        state = state * jnp.exp(t) + s
        total = total + t
    exact[...] = state
    heads = key_cols // CUE_WIDTH
    pack(out, state, total, against(asking(question, 8), state)[:heads])


def final_kernel(question, mine, other, exact, cache, read, *, bit):
    heads, kept, _ = cache.shape
    key_cols = question.shape[1]
    earlier = lax.bitwise_and(lax.axis_index("sp"), bit) == 0
    s_m, l_m, tail_m = unpack(mine, key_cols)
    s_o, l_o, tail_o = unpack(other, key_cols)
    fading = jnp.exp(jnp.where(earlier, l_o, l_m))
    first = jnp.where(earlier, s_m, s_o) * fading
    state = jnp.where(earlier, exact[...] * fading + s_o, first + exact[...])
    rows = heads * kept
    rows += -rows % 8
    row = lax.broadcasted_iota(jnp.int32, (rows, key_cols), 0)
    lane = lax.broadcasted_iota(jnp.int32, (rows, key_cols), 1)
    start = lax.axis_index("sp") * kept
    column = lax.div(row, kept) * CUE_WIDTH + start + lax.rem(row, kept)
    chosen = ((row < heads * kept) & (lane == column)).astype(F32)
    result = against(chosen, state)
    for h in range(heads):
        cache[h] = result[h * kept : (h + 1) * kept].astype(BF16)
    heard = against(asking(question, 8), first)[:heads]
    heard = heard + heard_of(jnp.where(earlier, tail_o, tail_m), heads)
    mean = jnp.mean(heard * heard, axis=-1, keepdims=True)
    read[...] = (heard * lax.rsqrt(mean + 1.0)).astype(BF16)


VM = pl.BlockSpec(memory_space=pltpu.VMEM)


def call(kernel, out_shape, in_specs, scratch=(), flops=0):
    return pl.pallas_call(
        kernel,
        out_shape=out_shape,
        in_specs=in_specs,
        out_specs=jax.tree.map(lambda _: VM, out_shape),
        scratch_shapes=list(scratch),
        cost_estimate=pl.CostEstimate(flops=flops, bytes_accessed=0, transcendentals=0),
        compiler_params=pltpu.CompilerParams(vmem_limit_bytes=VMEM_LIMIT),
    )


def whole(sp, tp, tokens, wk, wv, wd, decay_offset, fresh_question):
    rows, width = tokens.shape
    key_cols, value_cols = wk.shape[1], wv.shape[1]
    heads = key_cols // CUE_WIDTH
    cols = 2 * key_cols + value_cols
    log_length = math.log(rows * tp * sp)
    offset = decay_offset.reshape(1, key_cols)
    question = fresh_question.reshape(1, key_cols)
    sds = jax.ShapeDtypeStruct
    state_sds = sds((DV, key_cols), F32)
    total_sds = sds((1, key_cols), F32)

    edges = [rows * sum(ROW_PARTS[:n]) // sum(ROW_PARTS) for n in range(len(ROW_PARTS) + 1)]
    cuts = list(zip(edges[:-1], edges[1:]))
    far = {}
    for bit in range(1, tp // 2):
        for part, (lo, hi) in enumerate(cuts):
            far[bit, part] = lax.ppermute(tokens[lo:hi], "tp", swap(tp, 2 * bit))
    sibling = lax.ppermute(tokens, "tp", swap(tp, 1))

    s_near, l_near = call(
        functools.partial(near_kernel, log_length=log_length),
        (state_sds, total_sds),
        [VM] * 6,
        flops=4 * rows * width * cols,
    )(tokens, sibling, wk, wv, wd, offset)

    blocks, states, totals = [None], [s_near], [l_near]
    pairs = {}
    for bit, part in far:
        pairs[bit, part] = (far[bit, part], lax.ppermute(far[bit, part], "tp", swap(tp, 1)))
    last = (tp // 2 - 1, len(cuts) - 1)
    for bit in range(1, tp // 2):
        taken = [key for key in pairs if key[0] == bit and key != last]
        inputs = [x for key in taken for x in pairs[key]]
        count = len(inputs)
        outs = call(
            functools.partial(early_kernel, log_length=log_length, blocks=count),
            (state_sds,) * count + (total_sds,) * count,
            [VM] * (count + 4),
            flops=2 * sum(x.shape[0] for x in inputs) * width * cols,
        )(*inputs, wk, wv, wd, offset)
        blocks += [key + (same,) for key in taken for same in (True, False)]
        states += outs[:count]
        totals += outs[count:]
    payload = call(
        functools.partial(
            late_kernel,
            log_length=log_length,
            blocks=tuple(blocks),
            here=last,
            parts=len(cuts),
        ),
        payload_sds(heads),
        [VM] * (6 + 2 * len(blocks)),
        flops=4 * pairs[last][0].shape[0] * width * cols,
    )(*pairs[last], wk, wv, wd, offset, *states, *totals)

    bits = [1 << n for n in range(sp.bit_length() - 1)]
    while len(bits) > 1:
        take = 2 if len(bits) > 2 else 1
        group, bits = bits[:take], bits[take:]
        others = []
        for k in range(1, 2**take):
            far_bits = sum(b for n, b in enumerate(group) if k >> n & 1)
            others.append(lax.ppermute(payload, "sp", swap(sp, far_bits)))
        payload, exact = call(
            functools.partial(merge_kernel, bits=tuple(group)),
            (payload_sds(heads), state_sds),
            [VM] * (2 + len(others)),
        )(question, payload, *others)
    other = lax.ppermute(payload, "sp", swap(sp, bits[0]))
    return call(
        functools.partial(final_kernel, bit=bits[0]),
        (sds((heads, CUE_WIDTH // sp, DV), BF16), sds((heads, DV), BF16)),
        [VM] * 4,
    )(question, payload, other, exact)


def solution(mesh):
    sp, tp = mesh.shape["sp"], mesh.shape["tp"]
    in_specs = (
        P(("sp", "tp"), None),
        P(None, "tp"),
        P(None, "tp"),
        P(None, "tp"),
        P("tp"),
        P("tp", None),
    )
    out_specs = (P("tp", "sp", None), P("tp", None))
    return jax.shard_map(
        functools.partial(whole, sp, tp),
        mesh=mesh,
        in_specs=in_specs,
        out_specs=out_specs,
        check_vma=False,
    )
```

```python
import functools
import math

import jax
import jax.numpy as jnp
from jax import lax
from jax.experimental import pallas as pl
from jax.experimental.pallas import tpu as pltpu
from jax.sharding import PartitionSpec as P


CUE_WIDTH = 64
DV = 128
DECAY_TAU = 16.0
ROW_PARTS = (3, 8, 5)
VMEM_LIMIT = 8 * 1024 * 1024


F32 = jnp.float32
BF16 = jnp.bfloat16
EXACT = lax.Precision.HIGHEST


def swap(count, bit):
    return [(i, i ^ bit) for i in range(count)]


def project(x, wk, wv, wd, offset, log_length):
    keys = jnp.dot(x, wk[...], preferred_element_type=F32).astype(BF16)
    values = jnp.dot(x, wv[...], preferred_element_type=F32).astype(BF16)
    pre = jnp.dot(x, wd[...], preferred_element_type=F32)
    z = pre + offset + log_length
    log_decay = (jnp.minimum(z, 0.0) - jnp.log1p(jnp.exp(-jnp.abs(z)))) / DECAY_TAU
    return keys, values, log_decay


def later_within(log_decay, sizes):
    rows = log_decay.shape[0]
    i = lax.broadcasted_iota(jnp.int32, (rows, rows), 0)
    j = lax.broadcasted_iota(jnp.int32, (rows, rows), 1)
    mask = j > i
    edge = 0
    for size in sizes[:-1]:
        edge += size
        mask = mask & ((i >= edge) == (j >= edge))
    return jnp.dot(mask.astype(F32), log_decay, precision=EXACT, preferred_element_type=F32)


def weigh(keys, after):
    exact = keys.astype(F32) * jnp.exp(after)
    high = exact.astype(BF16)
    return high, (exact - high.astype(F32)).astype(BF16)


def outer(values, weighted):
    high, low = weighted
    heads = high.shape[1] // CUE_WIDTH
    group = min(2, heads)
    cols = group * CUE_WIDTH
    parts = []
    for g in range(heads // group):
        w = jnp.concatenate([p[:, g * cols : (g + 1) * cols] for p in (high, low)], axis=1)
        v = values[:, g * group * DV : (g + 1) * group * DV]
        full = lax.dot_general(v, w, (((0,), (0,)), ((), ())), preferred_element_type=F32)
        full = full[:, :cols] + full[:, cols:]
        kept = full[:DV]
        if group == 2:
            lane = lax.broadcasted_iota(jnp.int32, kept.shape, 1)
            kept = jnp.where(lane < CUE_WIDTH, kept, full[DV:])
        parts.append(kept)
    return parts[0] if len(parts) == 1 else jnp.concatenate(parts, axis=1)


def payload_sds(heads):
    pad = -(3 + 3 * heads) % 16
    width = max(heads * CUE_WIDTH, DV)
    return jax.ShapeDtypeStruct((DV + 3 + 3 * heads + pad, width), BF16)


def split(exact):
    parts, rest = [], exact
    for _ in range(3):
        parts.append(rest.astype(BF16).astype(F32))
        rest = rest - parts[-1]
    return parts


def widen(x, width):
    extra = width - x.shape[1]
    return jnp.concatenate([x, jnp.zeros((x.shape[0], extra), x.dtype)], axis=1) if extra else x


def pack(out, state, total, heard=None):
    width = out.shape[1]
    rows = [widen(p, width) for p in split(total)]
    if heard is not None:
        for part in split(heard):
            part = widen(part, width)
            rows += [part[h : h + 1] for h in range(part.shape[0])]
    row = lax.broadcasted_iota(jnp.int32, (out.shape[0] - DV, width), 0)
    tail = jnp.zeros(row.shape, F32)
    for n, value in enumerate(rows):
        tail = jnp.where(row == n, value, tail)
    out[:DV, :] = widen(state.astype(BF16), width)
    out[DV:, :] = tail.astype(BF16)


def unpack(ref, key_cols):
    tail = ref[DV:, :].astype(F32)
    total = tail[0:1] + tail[1:2] + tail[2:3]
    return ref[:DV, :key_cols].astype(F32), total[:, :key_cols], tail


def heard_of(tail, heads):
    parts = [tail[3 + n * heads : 3 + (n + 1) * heads, :DV] for n in range(3)]
    return parts[0] + parts[1] + parts[2]


def ask_kernel(question, out):
    row = lax.broadcasted_iota(jnp.int32, out.shape, 0)
    lane = lax.broadcasted_iota(jnp.int32, out.shape, 1)
    heads = question.shape[0]
    asked = jnp.concatenate([question[...].astype(F32)] * heads, axis=1) * CUE_WIDTH ** (-0.5)
    if out.shape[0] > heads:
        spare = jnp.zeros((out.shape[0] - heads, out.shape[1]), F32)
        asked = jnp.concatenate([asked, spare], axis=0)
    out[...] = jnp.where(lax.div(lane, CUE_WIDTH) == row, asked, 0.0)


def against(left, state):
    return lax.dot_general(
        left, state, (((1,), (1,)), ((), ())), precision=EXACT, preferred_element_type=F32
    )


def cut_kernel(tokens, *refs, cuts):
    sems = refs[-1]
    copies = [
        pltpu.make_async_copy(tokens.at[lo:hi, :], out, sems.at[n])
        for n, ((lo, hi), out) in enumerate(zip(cuts, refs))
    ]
    for copy in copies:
        copy.start()
    for copy in copies:
        copy.wait()


def near_kernel(x0, x1, wk, wv, wd, off, s_out, l_out, *, log_length):
    core = lax.rem(lax.axis_index("tp"), 2)
    rows = x0.shape[0]
    x = jnp.concatenate([x0[...], x1[...]], axis=0)
    keys, values, log_decay = project(x, wk, wv, wd, off[...], log_length)
    after = later_within(log_decay, [rows, rows])
    own = after[0:1] + log_decay[0:1]
    sib = after[rows : rows + 1] + log_decay[rows : rows + 1]
    own_tail = jnp.where(core == 0, sib, 0.0)
    sib_tail = jnp.where(core == 0, 0.0, own)
    row = lax.broadcasted_iota(jnp.int32, after.shape, 0)
    after = after + jnp.where(row < rows, own_tail, sib_tail)
    s_out[...] = outer(values, weigh(keys, after))
    l_out[...] = own + sib


def early_kernel(*refs, log_length, blocks):
    wk, wv, wd, off = refs[blocks : blocks + 4]
    outs = refs[blocks + 4 :]
    sizes = [ref.shape[0] for ref in refs[:blocks]]
    x = jnp.concatenate([ref[...] for ref in refs[:blocks]], axis=0)
    keys, values, log_decay = project(x, wk, wv, wd, off[...], log_length)
    after = later_within(log_decay, sizes)
    weighted = weigh(keys, after)
    lo = 0
    for n, size in enumerate(sizes):
        hi = lo + size
        outs[n][...] = outer(values[lo:hi], [w[lo:hi] for w in weighted])
        outs[blocks + n][...] = after[lo : lo + 1] + log_decay[lo : lo + 1]
        lo = hi


def late_kernel(xa, xb, wk, wv, wd, off, *refs, log_length, blocks, here, parts):
    states = refs[: len(blocks)]
    totals = refs[len(blocks) : 2 * len(blocks)]
    out = refs[2 * len(blocks)]
    place = lax.axis_index("tp")
    core = lax.rem(place, 2)
    chip = lax.div(place, 2)
    rows = xa.shape[0]

    def position(block):
        if block is None:
            return chip * (2 * parts)
        bit, part, same = block
        parity = core if same else 1 - core
        return lax.bitwise_xor(chip, bit) * (2 * parts) + parity * parts + part

    x = jnp.concatenate([xa[...], xb[...]], axis=0)
    keys, values, log_decay = project(x, wk, wv, wd, off[...], log_length)
    after = later_within(log_decay, [rows, rows])
    own = [
        after[0:1] + log_decay[0:1],
        after[rows : rows + 1] + log_decay[rows : rows + 1],
    ]
    every = [(position(b), totals[n][...]) for n, b in enumerate(blocks)]
    mine = [position(here + (True,)), position(here + (False,))]
    every += list(zip(mine, own))

    def later_of(pos):
        acc = jnp.zeros_like(own[0])
        for p, t in every:
            acc = acc + jnp.where(p > pos, t, 0.0)
        return acc

    row = lax.broadcasted_iota(jnp.int32, after.shape, 0)
    after = after + jnp.where(row < rows, later_of(mine[0]), later_of(mine[1]))
    state = outer(values, weigh(keys, after))
    total = own[0] + own[1]
    for n in range(len(blocks)):
        pos, t = every[n]
        state = state + states[n][...] * jnp.exp(later_of(pos))
        total = total + t
    pack(out, state, total)


def merge_kernel(asked, *refs, bits):
    count = 2 ** len(bits)
    out, exact = refs[count:]
    key_cols = asked.shape[1]
    parts = [unpack(ref, key_cols)[:2] for ref in refs[:count]]
    for n, bit in enumerate(bits):
        turned = lax.bitwise_and(lax.axis_index("sp"), bit) != 0
        parts = [
            tuple(jnp.where(turned, x, y) for x, y in zip(parts[k ^ (1 << n)], parts[k]))
            for k in range(count)
        ]
    state, total = parts[0]
    for s, t in parts[1:]:
        state = state * jnp.exp(t) + s
        total = total + t
    exact[...] = state
    heads = key_cols // CUE_WIDTH
    pack(out, state, total, against(asked[...], state)[:heads])


def final_kernel(asked, mine, other, exact, cache, read, *, bit):
    heads, kept, _ = cache.shape
    key_cols = asked.shape[1]
    earlier = lax.bitwise_and(lax.axis_index("sp"), bit) == 0
    s_m, l_m, tail_m = unpack(mine, key_cols)
    s_o, l_o, tail_o = unpack(other, key_cols)
    fading = jnp.exp(jnp.where(earlier, l_o, l_m))
    first = jnp.where(earlier, s_m, s_o) * fading
    state = jnp.where(earlier, exact[...] * fading + s_o, first + exact[...])
    rows = heads * kept
    rows += -rows % 8
    row = lax.broadcasted_iota(jnp.int32, (rows, key_cols), 0)
    lane = lax.broadcasted_iota(jnp.int32, (rows, key_cols), 1)
    start = lax.axis_index("sp") * kept
    column = lax.div(row, kept) * CUE_WIDTH + start + lax.rem(row, kept)
    chosen = ((row < heads * kept) & (lane == column)).astype(F32)
    result = against(chosen, state)
    for h in range(heads):
        cache[h] = result[h * kept : (h + 1) * kept].astype(BF16)
    heard = against(asked[...], first)[:heads]
    heard = heard + heard_of(jnp.where(earlier, tail_o, tail_m), heads)
    mean = jnp.mean(heard * heard, axis=-1, keepdims=True)
    read[...] = (heard * lax.rsqrt(mean + 1.0)).astype(BF16)


VM = pl.BlockSpec(memory_space=pltpu.VMEM)


def call(kernel, out_shape, in_specs, scratch=(), flops=0):
    return pl.pallas_call(
        kernel,
        out_shape=out_shape,
        in_specs=in_specs,
        out_specs=jax.tree.map(lambda _: VM, out_shape),
        scratch_shapes=list(scratch),
        cost_estimate=pl.CostEstimate(flops=flops, bytes_accessed=0, transcendentals=0),
        compiler_params=pltpu.CompilerParams(vmem_limit_bytes=VMEM_LIMIT),
    )


def whole(sp, tp, tokens, wk, wv, wd, decay_offset, fresh_question):
    rows, width = tokens.shape
    key_cols, value_cols = wk.shape[1], wv.shape[1]
    heads = key_cols // CUE_WIDTH
    cols = 2 * key_cols + value_cols
    log_length = math.log(rows * tp * sp)
    offset = decay_offset.reshape(1, key_cols)
    sds = jax.ShapeDtypeStruct
    state_sds = sds((DV, key_cols), F32)
    total_sds = sds((1, key_cols), F32)

    edges = [rows * sum(ROW_PARTS[:n]) // sum(ROW_PARTS) for n in range(len(ROW_PARTS) + 1)]
    cuts = list(zip(edges[:-1], edges[1:]))
    held = pltpu.with_memory_space_constraint(tokens, pltpu.HBM)
    pieces = []
    for some in (cuts[:1], cuts[1:]):
        pieces += call(
            functools.partial(cut_kernel, cuts=tuple(some)),
            tuple(pltpu.VMEM((hi - lo, width), BF16) for lo, hi in some),
            [pl.BlockSpec(memory_space=pltpu.HBM)],
            [pltpu.SemaphoreType.DMA((len(some),))],
        )(held)
    far = {}
    for bit in range(1, tp // 2):
        for part, piece in enumerate(pieces):
            far[bit, part] = lax.ppermute(piece, "tp", swap(tp, 2 * bit))
    sibling = lax.ppermute(tokens, "tp", swap(tp, 1))

    s_near, l_near = call(
        functools.partial(near_kernel, log_length=log_length),
        (state_sds, total_sds),
        [VM] * 6,
        flops=4 * rows * width * cols,
    )(tokens, sibling, wk, wv, wd, offset)

    asked = call(ask_kernel, sds((heads + -heads % 8, key_cols), F32), [VM])(fresh_question)

    blocks, states, totals = [None], [s_near], [l_near]
    pairs = {}
    for bit, part in far:
        pairs[bit, part] = (far[bit, part], lax.ppermute(far[bit, part], "tp", swap(tp, 1)))
    last = (tp // 2 - 1, len(cuts) - 1)
    for bit in range(1, tp // 2):
        taken = [key for key in pairs if key[0] == bit and key != last]
        inputs = [x for key in taken for x in pairs[key]]
        count = len(inputs)
        outs = call(
            functools.partial(early_kernel, log_length=log_length, blocks=count),
            (state_sds,) * count + (total_sds,) * count,
            [VM] * (count + 4),
            flops=2 * sum(x.shape[0] for x in inputs) * width * cols,
        )(*inputs, wk, wv, wd, offset)
        blocks += [key + (same,) for key in taken for same in (True, False)]
        states += outs[:count]
        totals += outs[count:]
    payload = call(
        functools.partial(
            late_kernel,
            log_length=log_length,
            blocks=tuple(blocks),
            here=last,
            parts=len(cuts),
        ),
        payload_sds(heads),
        [VM] * (6 + 2 * len(blocks)),
        flops=4 * pairs[last][0].shape[0] * width * cols,
    )(*pairs[last], wk, wv, wd, offset, *states, *totals)

    bits = [1 << n for n in range(sp.bit_length() - 1)]
    while len(bits) > 1:
        take = 2 if len(bits) > 2 else 1
        group, bits = bits[:take], bits[take:]
        others = []
        for k in range(1, 2**take):
            far_bits = sum(b for n, b in enumerate(group) if k >> n & 1)
            others.append(lax.ppermute(payload, "sp", swap(sp, far_bits)))
        payload, exact = call(
            functools.partial(merge_kernel, bits=tuple(group)),
            (payload_sds(heads), state_sds),
            [VM] * (2 + len(others)),
        )(asked, payload, *others)
    other = lax.ppermute(payload, "sp", swap(sp, bits[0]))
    return call(
        functools.partial(final_kernel, bit=bits[0]),
        (sds((heads, CUE_WIDTH // sp, DV), BF16), sds((heads, DV), BF16)),
        [VM] * 4,
    )(asked, payload, other, exact)


def solution(mesh):
    sp, tp = mesh.shape["sp"], mesh.shape["tp"]
    in_specs = (
        P(("sp", "tp"), None),
        P(None, "tp"),
        P(None, "tp"),
        P(None, "tp"),
        P("tp"),
        P("tp", None),
    )
    out_specs = (P("tp", "sp", None), P("tp", None))
    return jax.shard_map(
        functools.partial(whole, sp, tp),
        mesh=mesh,
        in_specs=in_specs,
        out_specs=out_specs,
        check_vma=False,
    )
```

```python
import functools
import math

import jax
import jax.numpy as jnp
from jax import lax
from jax.experimental import pallas as pl
from jax.experimental.pallas import tpu as pltpu
from jax.sharding import PartitionSpec as P


CUE_WIDTH = 64
DV = 128
DECAY_TAU = 16.0
ROW_PARTS = (3, 8, 3, 2)
LATE = 2
VMEM_LIMIT = 8 * 1024 * 1024


F32 = jnp.float32
BF16 = jnp.bfloat16
EXACT = lax.Precision.HIGHEST


def swap(count, bit):
    return [(i, i ^ bit) for i in range(count)]


def project(x, wk, wv, wd, offset, log_length):
    keys = jnp.dot(x, wk[...], preferred_element_type=F32).astype(BF16)
    values = jnp.dot(x, wv[...], preferred_element_type=F32).astype(BF16)
    pre = jnp.dot(x, wd[...], preferred_element_type=F32)
    z = pre + offset + log_length
    log_decay = (jnp.minimum(z, 0.0) - jnp.log1p(jnp.exp(-jnp.abs(z)))) / DECAY_TAU
    return keys, values, log_decay


def later_within(log_decay, sizes):
    rows = log_decay.shape[0]
    i = lax.broadcasted_iota(jnp.int32, (rows, rows), 0)
    j = lax.broadcasted_iota(jnp.int32, (rows, rows), 1)
    mask = j > i
    edge = 0
    for size in sizes[:-1]:
        edge += size
        mask = mask & ((i >= edge) == (j >= edge))
    return jnp.dot(mask.astype(F32), log_decay, precision=EXACT, preferred_element_type=F32)


def weigh(keys, after):
    exact = keys.astype(F32) * jnp.exp(after)
    high = exact.astype(BF16)
    return high, (exact - high.astype(F32)).astype(BF16)


def outer(values, weighted):
    high, low = weighted
    heads = high.shape[1] // CUE_WIDTH
    group = min(2, heads)
    cols = group * CUE_WIDTH
    parts = []
    for g in range(heads // group):
        w = jnp.concatenate([p[:, g * cols : (g + 1) * cols] for p in (high, low)], axis=1)
        v = values[:, g * group * DV : (g + 1) * group * DV]
        full = lax.dot_general(v, w, (((0,), (0,)), ((), ())), preferred_element_type=F32)
        full = full[:, :cols] + full[:, cols:]
        kept = full[:DV]
        if group == 2:
            lane = lax.broadcasted_iota(jnp.int32, kept.shape, 1)
            kept = jnp.where(lane < CUE_WIDTH, kept, full[DV:])
        parts.append(kept)
    return parts[0] if len(parts) == 1 else jnp.concatenate(parts, axis=1)


def payload_sds(heads, heard):
    rows = 3 + 3 * heads if heard else 3
    width = max(heads * CUE_WIDTH, DV)
    return jax.ShapeDtypeStruct((DV + rows + -rows % 8, width), BF16)


def split(exact):
    parts, rest = [], exact
    for _ in range(3):
        parts.append(rest.astype(BF16).astype(F32))
        rest = rest - parts[-1]
    return parts


def widen(x, width):
    extra = width - x.shape[1]
    return jnp.concatenate([x, jnp.zeros((x.shape[0], extra), x.dtype)], axis=1) if extra else x


def pack(out, state, total, heard=None):
    width = out.shape[1]
    rows = [widen(p, width) for p in split(total)]
    if heard is not None:
        for part in split(heard):
            part = widen(part, width)
            rows += [part[h : h + 1] for h in range(part.shape[0])]
    row = lax.broadcasted_iota(jnp.int32, (out.shape[0] - DV, width), 0)
    tail = jnp.zeros(row.shape, F32)
    for n, value in enumerate(rows):
        tail = jnp.where(row == n, value, tail)
    out[:DV, :] = widen(state.astype(BF16), width)
    out[DV:, :] = tail.astype(BF16)


def unpack(ref, key_cols):
    tail = ref[DV:, :].astype(F32)
    total = tail[0:1] + tail[1:2] + tail[2:3]
    return ref[:DV, :key_cols].astype(F32), total[:, :key_cols], tail


def heard_of(tail, heads):
    parts = [tail[3 + n * heads : 3 + (n + 1) * heads, :DV] for n in range(3)]
    return parts[0] + parts[1] + parts[2]


def ask_kernel(question, out):
    row = lax.broadcasted_iota(jnp.int32, out.shape, 0)
    lane = lax.broadcasted_iota(jnp.int32, out.shape, 1)
    heads = question.shape[0]
    asked = jnp.concatenate([question[...].astype(F32)] * heads, axis=1) * CUE_WIDTH ** (-0.5)
    if out.shape[0] > heads:
        spare = jnp.zeros((out.shape[0] - heads, out.shape[1]), F32)
        asked = jnp.concatenate([asked, spare], axis=0)
    out[...] = jnp.where(lax.div(lane, CUE_WIDTH) == row, asked, 0.0)


def against(left, state):
    return lax.dot_general(
        left, state, (((1,), (1,)), ((), ())), precision=EXACT, preferred_element_type=F32
    )


def cut_kernel(tokens, *refs, cuts):
    sems = refs[-1]
    copies = [
        pltpu.make_async_copy(tokens.at[lo:hi, :], out, sems.at[n])
        for n, ((lo, hi), out) in enumerate(zip(cuts, refs))
    ]
    for copy in copies:
        copy.start()
    for copy in copies:
        copy.wait()


def near_kernel(x0, x1, wk, wv, wd, off, s_out, l_out, *, log_length):
    core = lax.rem(lax.axis_index("tp"), 2)
    rows = x0.shape[0]
    x = jnp.concatenate([x0[...], x1[...]], axis=0)
    keys, values, log_decay = project(x, wk, wv, wd, off[...], log_length)
    after = later_within(log_decay, [rows, rows])
    own = after[0:1] + log_decay[0:1]
    sib = after[rows : rows + 1] + log_decay[rows : rows + 1]
    own_tail = jnp.where(core == 0, sib, 0.0)
    sib_tail = jnp.where(core == 0, 0.0, own)
    row = lax.broadcasted_iota(jnp.int32, after.shape, 0)
    after = after + jnp.where(row < rows, own_tail, sib_tail)
    s_out[...] = outer(values, weigh(keys, after))
    l_out[...] = own + sib


def early_kernel(*refs, log_length, blocks):
    wk, wv, wd, off = refs[blocks : blocks + 4]
    outs = refs[blocks + 4 :]
    sizes = [ref.shape[0] for ref in refs[:blocks]]
    x = jnp.concatenate([ref[...] for ref in refs[:blocks]], axis=0)
    keys, values, log_decay = project(x, wk, wv, wd, off[...], log_length)
    after = later_within(log_decay, sizes)
    weighted = weigh(keys, after)
    lo = 0
    for n, size in enumerate(sizes):
        hi = lo + size
        outs[n][...] = outer(values[lo:hi], [w[lo:hi] for w in weighted])
        outs[blocks + n][...] = after[lo : lo + 1] + log_decay[lo : lo + 1]
        lo = hi


def late_kernel(*refs, log_length, blocks, late, here, parts):
    x = jnp.concatenate([ref[...] for ref in refs[: 2 * late]], axis=0)
    wk, wv, wd, off = refs[2 * late : 2 * late + 4]
    refs = refs[2 * late + 4 :]
    states = refs[: len(blocks)]
    totals = refs[len(blocks) : 2 * len(blocks)]
    out = refs[2 * len(blocks)]
    place = lax.axis_index("tp")
    core = lax.rem(place, 2)
    chip = lax.div(place, 2)
    rows = x.shape[0] // 2

    def position(block):
        if block is None:
            return chip * (2 * parts)
        bit, part, same = block
        parity = core if same else 1 - core
        return lax.bitwise_xor(chip, bit) * (2 * parts) + parity * parts + part

    keys, values, log_decay = project(x, wk, wv, wd, off[...], log_length)
    after = later_within(log_decay, [rows, rows])
    own = [
        after[0:1] + log_decay[0:1],
        after[rows : rows + 1] + log_decay[rows : rows + 1],
    ]
    every = [(position(b), totals[n][...]) for n, b in enumerate(blocks)]
    mine = [position(here + (True,)), position(here + (False,))]
    every += list(zip(mine, own))

    def later_of(pos):
        acc = jnp.zeros_like(own[0])
        for p, t in every:
            acc = acc + jnp.where(p > pos, t, 0.0)
        return acc

    row = lax.broadcasted_iota(jnp.int32, after.shape, 0)
    after = after + jnp.where(row < rows, later_of(mine[0]), later_of(mine[1]))
    state = outer(values, weigh(keys, after))
    total = own[0] + own[1]
    for n in range(len(blocks)):
        pos, t = every[n]
        state = state + states[n][...] * jnp.exp(later_of(pos))
        total = total + t
    pack(out, state, total)


def merge_kernel(asked, *refs, bits):
    count = 2 ** len(bits)
    out, exact = refs[count:]
    key_cols = asked.shape[1]
    parts = [unpack(ref, key_cols)[:2] for ref in refs[:count]]
    for n, bit in enumerate(bits):
        turned = lax.bitwise_and(lax.axis_index("sp"), bit) != 0
        parts = [
            tuple(jnp.where(turned, x, y) for x, y in zip(parts[k ^ (1 << n)], parts[k]))
            for k in range(count)
        ]
    state, total = parts[0]
    for s, t in parts[1:]:
        state = state * jnp.exp(t) + s
        total = total + t
    exact[...] = state
    heads = key_cols // CUE_WIDTH
    last = out.shape[0] > DV + 8
    pack(out, state, total, against(asked[...], state)[:heads] if last else None)


def final_kernel(asked, mine, other, exact, cache, read, *, bit):
    heads, kept, _ = cache.shape
    key_cols = asked.shape[1]
    earlier = lax.bitwise_and(lax.axis_index("sp"), bit) == 0
    s_m, l_m, tail_m = unpack(mine, key_cols)
    s_o, l_o, tail_o = unpack(other, key_cols)
    fading = jnp.exp(jnp.where(earlier, l_o, l_m))
    first = jnp.where(earlier, s_m, s_o) * fading
    state = jnp.where(earlier, exact[...] * fading + s_o, first + exact[...])
    rows = heads * kept
    rows += -rows % 8
    row = lax.broadcasted_iota(jnp.int32, (rows, key_cols), 0)
    lane = lax.broadcasted_iota(jnp.int32, (rows, key_cols), 1)
    start = lax.axis_index("sp") * kept
    column = lax.div(row, kept) * CUE_WIDTH + start + lax.rem(row, kept)
    chosen = ((row < heads * kept) & (lane == column)).astype(F32)
    result = against(chosen, state)
    for h in range(heads):
        cache[h] = result[h * kept : (h + 1) * kept].astype(BF16)
    heard = against(asked[...], first)[:heads]
    heard = heard + heard_of(jnp.where(earlier, tail_o, tail_m), heads)
    mean = jnp.mean(heard * heard, axis=-1, keepdims=True)
    read[...] = (heard * lax.rsqrt(mean + 1.0)).astype(BF16)


VM = pl.BlockSpec(memory_space=pltpu.VMEM)


def call(kernel, out_shape, in_specs, scratch=(), flops=0):
    return pl.pallas_call(
        kernel,
        out_shape=out_shape,
        in_specs=in_specs,
        out_specs=jax.tree.map(lambda _: VM, out_shape),
        scratch_shapes=list(scratch),
        cost_estimate=pl.CostEstimate(flops=flops, bytes_accessed=0, transcendentals=0),
        compiler_params=pltpu.CompilerParams(vmem_limit_bytes=VMEM_LIMIT),
    )


def whole(sp, tp, tokens, wk, wv, wd, decay_offset, fresh_question):
    rows, width = tokens.shape
    key_cols, value_cols = wk.shape[1], wv.shape[1]
    heads = key_cols // CUE_WIDTH
    cols = 2 * key_cols + value_cols
    log_length = math.log(rows * tp * sp)
    offset = decay_offset.reshape(1, key_cols)
    sds = jax.ShapeDtypeStruct
    state_sds = sds((DV, key_cols), F32)
    total_sds = sds((1, key_cols), F32)

    edges = [rows * sum(ROW_PARTS[:n]) // sum(ROW_PARTS) for n in range(len(ROW_PARTS) + 1)]
    cuts = list(zip(edges[:-1], edges[1:]))
    held = pltpu.with_memory_space_constraint(tokens, pltpu.HBM)
    pieces = []
    for some in (cuts[:1], cuts[1:]):
        pieces += call(
            functools.partial(cut_kernel, cuts=tuple(some)),
            tuple(pltpu.VMEM((hi - lo, width), BF16) for lo, hi in some),
            [pl.BlockSpec(memory_space=pltpu.HBM)],
            [pltpu.SemaphoreType.DMA((len(some),))],
        )(held)
    far = {}
    for bit in range(1, tp // 2):
        for part, piece in enumerate(pieces):
            far[bit, part] = lax.ppermute(piece, "tp", swap(tp, 2 * bit))
    sibling = lax.ppermute(tokens, "tp", swap(tp, 1))

    s_near, l_near = call(
        functools.partial(near_kernel, log_length=log_length),
        (state_sds, total_sds),
        [VM] * 6,
        flops=4 * rows * width * cols,
    )(tokens, sibling, wk, wv, wd, offset)

    asked = call(ask_kernel, sds((heads + -heads % 8, key_cols), F32), [VM])(fresh_question)

    blocks, states, totals = [None], [s_near], [l_near]
    pairs = {}
    for bit, part in far:
        pairs[bit, part] = (far[bit, part], lax.ppermute(far[bit, part], "tp", swap(tp, 1)))
    early = len(cuts) - LATE
    last = [(tp // 2 - 1, early + n) for n in range(LATE)]
    for bit in range(1, tp // 2):
        taken = [key for key in pairs if key[0] == bit and key not in last]
        inputs = [x for key in taken for x in pairs[key]]
        count = len(inputs)
        outs = call(
            functools.partial(early_kernel, log_length=log_length, blocks=count),
            (state_sds,) * count + (total_sds,) * count,
            [VM] * (count + 4),
            flops=2 * sum(x.shape[0] for x in inputs) * width * cols,
        )(*inputs, wk, wv, wd, offset)
        blocks += [key + (same,) for key in taken for same in (True, False)]
        states += outs[:count]
        totals += outs[count:]
    payload = call(
        functools.partial(
            late_kernel,
            log_length=log_length,
            blocks=tuple(blocks),
            late=LATE,
            here=last[0],
            parts=len(cuts),
        ),
        payload_sds(heads, sp == 2),
        [VM] * (2 * LATE + 4 + 2 * len(blocks)),
        flops=4 * (edges[-1] - edges[early]) * width * cols,
    )(*(pairs[key][side] for side in (0, 1) for key in last), wk, wv, wd, offset, *states, *totals)

    bits = [1 << n for n in range(sp.bit_length() - 1)]
    while len(bits) > 1:
        take = 2 if len(bits) > 2 else 1
        group, bits = bits[:take], bits[take:]
        others = []
        for k in range(1, 2**take):
            far_bits = sum(b for n, b in enumerate(group) if k >> n & 1)
            others.append(lax.ppermute(payload, "sp", swap(sp, far_bits)))
        payload, exact = call(
            functools.partial(merge_kernel, bits=tuple(group)),
            (payload_sds(heads, len(bits) == 1), state_sds),
            [VM] * (2 + len(others)),
        )(asked, payload, *others)
    other = lax.ppermute(payload, "sp", swap(sp, bits[0]))
    return call(
        functools.partial(final_kernel, bit=bits[0]),
        (sds((heads, CUE_WIDTH // sp, DV), BF16), sds((heads, DV), BF16)),
        [VM] * 4,
    )(asked, payload, other, exact)


def solution(mesh):
    sp, tp = mesh.shape["sp"], mesh.shape["tp"]
    in_specs = (
        P(("sp", "tp"), None),
        P(None, "tp"),
        P(None, "tp"),
        P(None, "tp"),
        P("tp"),
        P("tp", None),
    )
    out_specs = (P("tp", "sp", None), P("tp", None))
    step = jax.shard_map(
        functools.partial(whole, sp, tp),
        mesh=mesh,
        in_specs=in_specs,
        out_specs=out_specs,
        check_vma=False,
    )
    bit = 1
    while 4 * bit < sp:
        bit *= 4
    return step
```

```python
import functools
import math

import jax
import jax.numpy as jnp
from jax import lax
from jax.experimental import pallas as pl
from jax.experimental.pallas import tpu as pltpu
from jax.sharding import PartitionSpec as P


CUE_WIDTH = 64
DV = 128
DECAY_TAU = 16.0
ROW_PARTS = (2, 3, 3)
COL_PARTS = (3, 1)
LATE = len(COL_PARTS)
VMEM_LIMIT = 8 * 1024 * 1024


F32 = jnp.float32
BF16 = jnp.bfloat16
EXACT = lax.Precision.HIGHEST


def swap(count, bit):
    return [(i, i ^ bit) for i in range(count)]


def products(x, weights, start=0):
    stop = start + x.shape[1]
    return [jnp.dot(x, w[start:stop, :], preferred_element_type=F32) for w in weights]


def project(sums, offset, log_length):
    keys, values, pre = sums
    z = pre + offset + log_length
    log_decay = (jnp.minimum(z, 0.0) - jnp.log1p(jnp.exp(-jnp.abs(z)))) / DECAY_TAU
    return keys.astype(BF16), values.astype(BF16), log_decay


def later_within(log_decay, sizes):
    rows = log_decay.shape[0]
    i = lax.broadcasted_iota(jnp.int32, (rows, rows), 0)
    j = lax.broadcasted_iota(jnp.int32, (rows, rows), 1)
    mask = j > i
    edge = 0
    for size in sizes[:-1]:
        edge += size
        mask = mask & ((i >= edge) == (j >= edge))
    return jnp.dot(mask.astype(F32), log_decay, precision=EXACT, preferred_element_type=F32)


def weigh(keys, after):
    exact = keys.astype(F32) * jnp.exp(after)
    high = exact.astype(BF16)
    return high, (exact - high.astype(F32)).astype(BF16)


def outer(values, weighted):
    high, low = weighted
    heads = high.shape[1] // CUE_WIDTH
    group = min(2, heads)
    cols = group * CUE_WIDTH
    parts = []
    for g in range(heads // group):
        w = jnp.concatenate([p[:, g * cols : (g + 1) * cols] for p in (high, low)], axis=1)
        v = values[:, g * group * DV : (g + 1) * group * DV]
        full = lax.dot_general(v, w, (((0,), (0,)), ((), ())), preferred_element_type=F32)
        full = full[:, :cols] + full[:, cols:]
        kept = full[:DV]
        if group == 2:
            lane = lax.broadcasted_iota(jnp.int32, kept.shape, 1)
            kept = jnp.where(lane < CUE_WIDTH, kept, full[DV:])
        parts.append(kept)
    return parts[0] if len(parts) == 1 else jnp.concatenate(parts, axis=1)


def payload_sds(heads, heard):
    rows = 3 + 3 * heads if heard else 3
    width = max(heads * CUE_WIDTH, DV)
    return jax.ShapeDtypeStruct((DV + rows + -rows % 8, width), BF16)


def split(exact):
    parts, rest = [], exact
    for _ in range(3):
        parts.append(rest.astype(BF16).astype(F32))
        rest = rest - parts[-1]
    return parts


def widen(x, width):
    extra = width - x.shape[1]
    return jnp.concatenate([x, jnp.zeros((x.shape[0], extra), x.dtype)], axis=1) if extra else x


def pack(out, state, total, heard=None):
    width = out.shape[1]
    rows = [widen(p, width) for p in split(total)]
    if heard is not None:
        for part in split(heard):
            part = widen(part, width)
            rows += [part[h : h + 1] for h in range(part.shape[0])]
    row = lax.broadcasted_iota(jnp.int32, (out.shape[0] - DV, width), 0)
    tail = jnp.zeros(row.shape, F32)
    for n, value in enumerate(rows):
        tail = jnp.where(row == n, value, tail)
    out[:DV, :] = widen(state.astype(BF16), width)
    out[DV:, :] = tail.astype(BF16)


def unpack(ref, key_cols):
    tail = ref[DV:, :].astype(F32)
    total = tail[0:1] + tail[1:2] + tail[2:3]
    return ref[:DV, :key_cols].astype(F32), total[:, :key_cols], tail


def heard_of(tail, heads):
    parts = [tail[3 + n * heads : 3 + (n + 1) * heads, :DV] for n in range(3)]
    return parts[0] + parts[1] + parts[2]


def ask_kernel(question, out):
    row = lax.broadcasted_iota(jnp.int32, out.shape, 0)
    lane = lax.broadcasted_iota(jnp.int32, out.shape, 1)
    heads = question.shape[0]
    asked = jnp.concatenate([question[...].astype(F32)] * heads, axis=1) * CUE_WIDTH ** (-0.5)
    if out.shape[0] > heads:
        spare = jnp.zeros((out.shape[0] - heads, out.shape[1]), F32)
        asked = jnp.concatenate([asked, spare], axis=0)
    out[...] = jnp.where(lax.div(lane, CUE_WIDTH) == row, asked, 0.0)


def against(left, state):
    return lax.dot_general(
        left, state, (((1,), (1,)), ((), ())), precision=EXACT, preferred_element_type=F32
    )


def cut_kernel(tokens, *refs, cuts):
    sems = refs[-1]
    copies = [
        pltpu.make_async_copy(tokens.at[lo:hi, left:right], out, sems.at[n])
        for n, ((lo, hi, left, right), out) in enumerate(zip(cuts, refs))
    ]
    for copy in copies:
        copy.start()
    for copy in copies:
        copy.wait()


def near_kernel(x0, x1, wk, wv, wd, off, s_out, l_out, *, log_length):
    core = lax.rem(lax.axis_index("tp"), 2)
    rows = x0.shape[0]
    x = jnp.concatenate([x0[...], x1[...]], axis=0)
    keys, values, log_decay = project(products(x, (wk, wv, wd)), off[...], log_length)
    after = later_within(log_decay, [rows, rows])
    own = after[0:1] + log_decay[0:1]
    sib = after[rows : rows + 1] + log_decay[rows : rows + 1]
    own_tail = jnp.where(core == 0, sib, 0.0)
    sib_tail = jnp.where(core == 0, 0.0, own)
    row = lax.broadcasted_iota(jnp.int32, after.shape, 0)
    after = after + jnp.where(row < rows, own_tail, sib_tail)
    s_out[...] = outer(values, weigh(keys, after))
    l_out[...] = own + sib


def early_kernel(*refs, log_length, pieces, split):
    sides = []
    for side in (refs[:pieces], refs[pieces : 2 * pieces]):
        whole = [ref[...] for ref in side]
        if split:
            whole = whole[:-LATE] + [jnp.concatenate(whole[-LATE:], axis=1)]
        sides.append(jnp.concatenate(whole, axis=0))
    wk, wv, wd, off, s_a, s_b, l_a, l_b = refs[2 * pieces :]
    rows = sides[0].shape[0]
    x = jnp.concatenate(sides, axis=0)
    keys, values, log_decay = project(products(x, (wk, wv, wd)), off[...], log_length)
    after = later_within(log_decay, [rows, rows])
    weighted = weigh(keys, after)
    s_a[...] = outer(values[:rows], [w[:rows] for w in weighted])
    s_b[...] = outer(values[rows:], [w[rows:] for w in weighted])
    l_a[...] = after[0:1] + log_decay[0:1]
    l_b[...] = after[rows : rows + 1] + log_decay[rows : rows + 1]


def partial_kernel(xa, xb, wk, wv, wd, *outs):
    x = jnp.concatenate([xa[...], xb[...]], axis=0)
    for out, value in zip(outs, products(x, (wk, wv, wd))):
        out[...] = value


def late_kernel(xa, xb, ks, vs, ds, wk, wv, wd, off, *refs, log_length, blocks, here, parts):
    states = refs[: len(blocks)]
    totals = refs[len(blocks) : 2 * len(blocks)]
    out = refs[2 * len(blocks)]
    place = lax.axis_index("tp")
    core = lax.rem(place, 2)
    chip = lax.div(place, 2)
    rows = xa.shape[0]

    def position(block):
        if block is None:
            return chip * (2 * parts)
        bit, part, same = block
        parity = core if same else 1 - core
        return lax.bitwise_xor(chip, bit) * (2 * parts) + parity * parts + part

    x = jnp.concatenate([xa[...], xb[...]], axis=0)
    more = products(x, (wk, wv, wd), wk.shape[0] - x.shape[1])
    sums = [s[...] + m for s, m in zip((ks, vs, ds), more)]
    keys, values, log_decay = project(sums, off[...], log_length)
    after = later_within(log_decay, [rows, rows])
    own = [
        after[0:1] + log_decay[0:1],
        after[rows : rows + 1] + log_decay[rows : rows + 1],
    ]
    every = [(position(b), totals[n][...]) for n, b in enumerate(blocks)]
    mine = [position(here + (True,)), position(here + (False,))]
    every += list(zip(mine, own))

    def later_of(pos):
        acc = jnp.zeros_like(own[0])
        for p, t in every:
            acc = acc + jnp.where(p > pos, t, 0.0)
        return acc

    row = lax.broadcasted_iota(jnp.int32, after.shape, 0)
    after = after + jnp.where(row < rows, later_of(mine[0]), later_of(mine[1]))
    state = outer(values, weigh(keys, after))
    total = own[0] + own[1]
    for n in range(len(blocks)):
        pos, t = every[n]
        state = state + states[n][...] * jnp.exp(later_of(pos))
        total = total + t
    pack(out, state, total)


def merge_kernel(asked, *refs, bits):
    count = 2 ** len(bits)
    out, exact = refs[count:]
    key_cols = asked.shape[1]
    parts = [unpack(ref, key_cols)[:2] for ref in refs[:count]]
    for n, bit in enumerate(bits):
        turned = lax.bitwise_and(lax.axis_index("sp"), bit) != 0
        parts = [
            tuple(jnp.where(turned, x, y) for x, y in zip(parts[k ^ (1 << n)], parts[k]))
            for k in range(count)
        ]
    state, total = parts[0]
    for s, t in parts[1:]:
        state = state * jnp.exp(t) + s
        total = total + t
    exact[...] = state
    heads = key_cols // CUE_WIDTH
    last = out.shape[0] > DV + 8
    pack(out, state, total, against(asked[...], state)[:heads] if last else None)


def final_kernel(asked, mine, other, exact, cache, read, *, bit):
    heads, kept, _ = cache.shape
    key_cols = asked.shape[1]
    earlier = lax.bitwise_and(lax.axis_index("sp"), bit) == 0
    s_m, l_m, tail_m = unpack(mine, key_cols)
    s_o, l_o, tail_o = unpack(other, key_cols)
    fading = jnp.exp(jnp.where(earlier, l_o, l_m))
    first = jnp.where(earlier, s_m, s_o) * fading
    state = jnp.where(earlier, exact[...] * fading + s_o, first + exact[...])
    rows = heads * kept
    rows += -rows % 8
    row = lax.broadcasted_iota(jnp.int32, (rows, key_cols), 0)
    lane = lax.broadcasted_iota(jnp.int32, (rows, key_cols), 1)
    start = lax.axis_index("sp") * kept
    column = lax.div(row, kept) * CUE_WIDTH + start + lax.rem(row, kept)
    chosen = ((row < heads * kept) & (lane == column)).astype(F32)
    result = against(chosen, state)
    for h in range(heads):
        cache[h] = result[h * kept : (h + 1) * kept].astype(BF16)
    heard = against(asked[...], first)[:heads]
    heard = heard + heard_of(jnp.where(earlier, tail_o, tail_m), heads)
    mean = jnp.mean(heard * heard, axis=-1, keepdims=True)
    read[...] = (heard * lax.rsqrt(mean + 1.0)).astype(BF16)


VM = pl.BlockSpec(memory_space=pltpu.VMEM)


def call(kernel, out_shape, in_specs, scratch=(), flops=0):
    return pl.pallas_call(
        kernel,
        out_shape=out_shape,
        in_specs=in_specs,
        out_specs=jax.tree.map(lambda _: VM, out_shape),
        scratch_shapes=list(scratch),
        cost_estimate=pl.CostEstimate(flops=flops, bytes_accessed=0, transcendentals=0),
        compiler_params=pltpu.CompilerParams(vmem_limit_bytes=VMEM_LIMIT),
    )


def whole(sp, tp, tokens, wk, wv, wd, decay_offset, fresh_question):
    rows, width = tokens.shape
    key_cols, value_cols = wk.shape[1], wv.shape[1]
    heads = key_cols // CUE_WIDTH
    cols = 2 * key_cols + value_cols
    log_length = math.log(rows * tp * sp)
    offset = decay_offset.reshape(1, key_cols)
    sds = jax.ShapeDtypeStruct
    state_sds = sds((DV, key_cols), F32)
    total_sds = sds((1, key_cols), F32)

    edges = [rows * sum(ROW_PARTS[:n]) // sum(ROW_PARTS) for n in range(len(ROW_PARTS) + 1)]
    sides = [width * sum(COL_PARTS[:n]) // sum(COL_PARTS) for n in range(LATE + 1)]
    cuts = [(lo, hi, 0, width) for lo, hi in zip(edges[:-2], edges[1:-1])]
    cuts += [(edges[-2], edges[-1], lo, hi) for lo, hi in zip(sides[:-1], sides[1:])]
    held = pltpu.with_memory_space_constraint(tokens, pltpu.HBM)
    pieces = []
    for some in (cuts[:1], cuts[1:]):
        pieces += call(
            functools.partial(cut_kernel, cuts=tuple(some)),
            tuple(pltpu.VMEM((h - l, r - c), BF16) for l, h, c, r in some),
            [pl.BlockSpec(memory_space=pltpu.HBM)],
            [pltpu.SemaphoreType.DMA((len(some),))],
        )(held)
    far = {}
    for bit in range(1, tp // 2):
        for part, piece in enumerate(pieces):
            far[bit, part] = lax.ppermute(piece, "tp", swap(tp, 2 * bit))
    sibling = lax.ppermute(tokens, "tp", swap(tp, 1))

    s_near, l_near = call(
        functools.partial(near_kernel, log_length=log_length),
        (state_sds, total_sds),
        [VM] * 6,
        flops=4 * rows * width * cols,
    )(tokens, sibling, wk, wv, wd, offset)

    asked = call(ask_kernel, sds((heads + -heads % 8, key_cols), F32), [VM])(fresh_question)

    blocks, states, totals = [None], [s_near], [l_near]
    pairs = {}
    for bit, part in far:
        pairs[bit, part] = (far[bit, part], lax.ppermute(far[bit, part], "tp", swap(tp, 1)))
    final_bit = tp // 2 - 1
    last = [pairs[final_bit, len(cuts) - LATE + n] for n in range(LATE)]
    for bit in range(1, tp // 2):
        taken = [pairs[bit, n] for n in range(len(cuts) - (LATE if bit == final_bit else 0))]
        inputs = [pair[side] for side in (0, 1) for pair in taken]
        far_rows = edges[-2] if bit == final_bit else rows
        s_a, s_b, l_a, l_b = call(
            functools.partial(
                early_kernel,
                log_length=log_length,
                pieces=len(taken),
                split=bit != final_bit,
            ),
            (state_sds, state_sds, total_sds, total_sds),
            [VM] * (len(inputs) + 4),
            flops=4 * far_rows * width * cols,
        )(*inputs, wk, wv, wd, offset)
        blocks += [(bit, 0, True), (bit, 0, False)]
        states += [s_a, s_b]
        totals += [l_a, l_b]
    late_rows = 2 * (edges[-1] - edges[-2])
    sums = call(
        partial_kernel,
        tuple(sds((late_rows, w.shape[1]), F32) for w in (wk, wv, wd)),
        [VM] * 5,
        flops=2 * late_rows * sides[1] * cols,
    )(*last[0], wk, wv, wd)
    payload = call(
        functools.partial(
            late_kernel, log_length=log_length, blocks=tuple(blocks), here=(final_bit, 1), parts=2
        ),
        payload_sds(heads, sp == 2),
        [VM] * (9 + 2 * len(blocks)),
        flops=2 * late_rows * (width - sides[1]) * cols,
    )(*last[1], *sums, wk, wv, wd, offset, *states, *totals)

    bits = [1 << n for n in range(sp.bit_length() - 1)]
    while len(bits) > 1:
        take = 2 if len(bits) > 2 else 1
        group, bits = bits[:take], bits[take:]
        others = []
        for k in range(1, 2**take):
            far_bits = sum(b for n, b in enumerate(group) if k >> n & 1)
            others.append(lax.ppermute(payload, "sp", swap(sp, far_bits)))
        payload, exact = call(
            functools.partial(merge_kernel, bits=tuple(group)),
            (payload_sds(heads, len(bits) == 1), state_sds),
            [VM] * (2 + len(others)),
        )(asked, payload, *others)
    other = lax.ppermute(payload, "sp", swap(sp, bits[0]))
    return call(
        functools.partial(final_kernel, bit=bits[0]),
        (sds((heads, CUE_WIDTH // sp, DV), BF16), sds((heads, DV), BF16)),
        [VM] * 4,
    )(asked, payload, other, exact)


def solution(mesh):
    sp, tp = mesh.shape["sp"], mesh.shape["tp"]
    in_specs = (
        P(("sp", "tp"), None),
        P(None, "tp"),
        P(None, "tp"),
        P(None, "tp"),
        P("tp"),
        P("tp", None),
    )
    out_specs = (P("tp", "sp", None), P("tp", None))
    return jax.shard_map(
        functools.partial(whole, sp, tp),
        mesh=mesh,
        in_specs=in_specs,
        out_specs=out_specs,
        check_vma=False,
    )
```

```python
import functools
import math

import jax
import jax.numpy as jnp
from jax import lax
from jax.experimental import pallas as pl
from jax.experimental.pallas import tpu as pltpu
from jax.sharding import PartitionSpec as P


CUE_WIDTH = 64
DV = 128
DECAY_TAU = 16.0
ROW_PARTS = (2, 3, 3)
COL_PARTS = (5, 3)
LATE = len(COL_PARTS)
VMEM_LIMIT = 8 * 1024 * 1024


F32 = jnp.float32
BF16 = jnp.bfloat16
EXACT = lax.Precision.HIGHEST


def swap(count, bit):
    return [(i, i ^ bit) for i in range(count)]


def products(x, weights, start=0):
    stop = start + x.shape[1]
    return [jnp.dot(x, w[start:stop, :], preferred_element_type=F32) for w in weights]


def project(sums, offset, log_length):
    keys, values, pre = sums
    z = pre + offset + log_length
    log_decay = (jnp.minimum(z, 0.0) - jnp.log1p(jnp.exp(-jnp.abs(z)))) / DECAY_TAU
    return keys.astype(BF16), values.astype(BF16), log_decay


def later_within(log_decay, sizes):
    rows = log_decay.shape[0]
    i = lax.broadcasted_iota(jnp.int32, (rows, rows), 0)
    j = lax.broadcasted_iota(jnp.int32, (rows, rows), 1)
    mask = j > i
    edge = 0
    for size in sizes[:-1]:
        edge += size
        mask = mask & ((i >= edge) == (j >= edge))
    return jnp.dot(mask.astype(F32), log_decay, precision=EXACT, preferred_element_type=F32)


def weigh(keys, after):
    exact = keys.astype(F32) * jnp.exp(after)
    high = exact.astype(BF16)
    return high, (exact - high.astype(F32)).astype(BF16)


def outer(values, weighted):
    high, low = weighted
    heads = high.shape[1] // CUE_WIDTH
    group = min(2, heads)
    cols = group * CUE_WIDTH
    parts = []
    for g in range(heads // group):
        w = jnp.concatenate([p[:, g * cols : (g + 1) * cols] for p in (high, low)], axis=1)
        v = values[:, g * group * DV : (g + 1) * group * DV]
        full = lax.dot_general(v, w, (((0,), (0,)), ((), ())), preferred_element_type=F32)
        full = full[:, :cols] + full[:, cols:]
        kept = full[:DV]
        if group == 2:
            lane = lax.broadcasted_iota(jnp.int32, kept.shape, 1)
            kept = jnp.where(lane < CUE_WIDTH, kept, full[DV:])
        parts.append(kept)
    return parts[0] if len(parts) == 1 else jnp.concatenate(parts, axis=1)


def payload_sds(heads, heard):
    rows = 3 + 3 * heads if heard else 3
    width = max(heads * CUE_WIDTH, DV)
    return jax.ShapeDtypeStruct((DV + rows + -rows % 8, width), BF16)


def split(exact):
    parts, rest = [], exact
    for _ in range(3):
        parts.append(rest.astype(BF16).astype(F32))
        rest = rest - parts[-1]
    return parts


def widen(x, width):
    extra = width - x.shape[1]
    return jnp.concatenate([x, jnp.zeros((x.shape[0], extra), x.dtype)], axis=1) if extra else x


def pack(out, state, total, heard=None):
    width = out.shape[1]
    rows = [widen(p, width) for p in split(total)]
    if heard is not None:
        for part in split(heard):
            part = widen(part, width)
            rows += [part[h : h + 1] for h in range(part.shape[0])]
    row = lax.broadcasted_iota(jnp.int32, (out.shape[0] - DV, width), 0)
    tail = jnp.zeros(row.shape, F32)
    for n, value in enumerate(rows):
        tail = jnp.where(row == n, value, tail)
    out[:DV, :] = widen(state.astype(BF16), width)
    out[DV:, :] = tail.astype(BF16)


def unpack(ref, key_cols):
    tail = ref[DV:, :].astype(F32)
    total = tail[0:1] + tail[1:2] + tail[2:3]
    return ref[:DV, :key_cols].astype(F32), total[:, :key_cols], tail


def heard_of(tail, heads):
    parts = [tail[3 + n * heads : 3 + (n + 1) * heads, :DV] for n in range(3)]
    return parts[0] + parts[1] + parts[2]


def ask_kernel(question, out):
    row = lax.broadcasted_iota(jnp.int32, out.shape, 0)
    lane = lax.broadcasted_iota(jnp.int32, out.shape, 1)
    heads = question.shape[0]
    asked = jnp.concatenate([question[...].astype(F32)] * heads, axis=1) * CUE_WIDTH ** (-0.5)
    if out.shape[0] > heads:
        spare = jnp.zeros((out.shape[0] - heads, out.shape[1]), F32)
        asked = jnp.concatenate([asked, spare], axis=0)
    out[...] = jnp.where(lax.div(lane, CUE_WIDTH) == row, asked, 0.0)


def against(left, state):
    return lax.dot_general(
        left, state, (((1,), (1,)), ((), ())), precision=EXACT, preferred_element_type=F32
    )


def cut_kernel(tokens, *refs, cuts):
    sems = refs[-1]
    copies = [
        pltpu.make_async_copy(tokens.at[lo:hi, left:right], out, sems.at[n])
        for n, ((lo, hi, left, right), out) in enumerate(zip(cuts, refs))
    ]
    for copy in copies:
        copy.start()
    for copy in copies:
        copy.wait()


def near_kernel(x0, x1, *refs, log_length):
    stored, off, kept, (s_out, l_out, sems) = refs[:3], refs[3], refs[4:7], refs[7:]
    loads = [pltpu.make_async_copy(h, v, sems.at[n]) for n, (h, v) in enumerate(zip(stored, kept))]
    for load in loads:
        load.start()
    core = lax.rem(lax.axis_index("tp"), 2)
    rows = x0.shape[0]
    x = jnp.concatenate([x0[...], x1[...]], axis=0)
    sums = []
    for load, w in zip(loads, kept):
        load.wait()
        sums += products(x, [w])
    keys, values, log_decay = project(sums, off[...], log_length)
    after = later_within(log_decay, [rows, rows])
    own = after[0:1] + log_decay[0:1]
    sib = after[rows : rows + 1] + log_decay[rows : rows + 1]
    own_tail = jnp.where(core == 0, sib, 0.0)
    sib_tail = jnp.where(core == 0, 0.0, own)
    row = lax.broadcasted_iota(jnp.int32, after.shape, 0)
    after = after + jnp.where(row < rows, own_tail, sib_tail)
    s_out[...] = outer(values, weigh(keys, after))
    l_out[...] = own + sib


def early_kernel(*refs, log_length, pieces, split):
    sides = []
    for side in (refs[:pieces], refs[pieces : 2 * pieces]):
        whole = [ref[...] for ref in side]
        if split:
            whole = whole[:-LATE] + [jnp.concatenate(whole[-LATE:], axis=1)]
        sides.append(jnp.concatenate(whole, axis=0))
    wk, wv, wd, off, s_a, s_b, l_a, l_b = refs[2 * pieces :]
    rows = sides[0].shape[0]
    x = jnp.concatenate(sides, axis=0)
    keys, values, log_decay = project(products(x, (wk, wv, wd)), off[...], log_length)
    after = later_within(log_decay, [rows, rows])
    weighted = weigh(keys, after)
    s_a[...] = outer(values[:rows], [w[:rows] for w in weighted])
    s_b[...] = outer(values[rows:], [w[rows:] for w in weighted])
    l_a[...] = after[0:1] + log_decay[0:1]
    l_b[...] = after[rows : rows + 1] + log_decay[rows : rows + 1]


def partial_kernel(xa, xb, wk, wv, wd, *outs):
    x = jnp.concatenate([xa[...], xb[...]], axis=0)
    for out, value in zip(outs, products(x, (wk, wv, wd))):
        out[...] = value


def late_kernel(xa, xb, ks, vs, ds, wk, wv, wd, off, *refs, log_length, blocks, here, parts):
    states = refs[: len(blocks)]
    totals = refs[len(blocks) : 2 * len(blocks)]
    out = refs[2 * len(blocks)]
    place = lax.axis_index("tp")
    core = lax.rem(place, 2)
    chip = lax.div(place, 2)
    rows = xa.shape[0]

    def position(block):
        if block is None:
            return chip * (2 * parts)
        bit, part, same = block
        parity = core if same else 1 - core
        return lax.bitwise_xor(chip, bit) * (2 * parts) + parity * parts + part

    x = jnp.concatenate([xa[...], xb[...]], axis=0)
    more = products(x, (wk, wv, wd), wk.shape[0] - x.shape[1])
    sums = [s[...] + m for s, m in zip((ks, vs, ds), more)]
    keys, values, log_decay = project(sums, off[...], log_length)
    after = later_within(log_decay, [rows, rows])
    own = [
        after[0:1] + log_decay[0:1],
        after[rows : rows + 1] + log_decay[rows : rows + 1],
    ]
    every = [(position(b), totals[n][...]) for n, b in enumerate(blocks)]
    mine = [position(here + (True,)), position(here + (False,))]
    every += list(zip(mine, own))

    def later_of(pos):
        acc = jnp.zeros_like(own[0])
        for p, t in every:
            acc = acc + jnp.where(p > pos, t, 0.0)
        return acc

    row = lax.broadcasted_iota(jnp.int32, after.shape, 0)
    after = after + jnp.where(row < rows, later_of(mine[0]), later_of(mine[1]))
    state = outer(values, weigh(keys, after))
    total = own[0] + own[1]
    for n in range(len(blocks)):
        pos, t = every[n]
        state = state + states[n][...] * jnp.exp(later_of(pos))
        total = total + t
    pack(out, state, total)


def merge_kernel(asked, *refs, bits):
    count = 2 ** len(bits)
    out, exact = refs[count:]
    key_cols = asked.shape[1]
    parts = [unpack(ref, key_cols)[:2] for ref in refs[:count]]
    for n, bit in enumerate(bits):
        turned = lax.bitwise_and(lax.axis_index("sp"), bit) != 0
        parts = [
            tuple(jnp.where(turned, x, y) for x, y in zip(parts[k ^ (1 << n)], parts[k]))
            for k in range(count)
        ]
    state, total = parts[0]
    for s, t in parts[1:]:
        state = state * jnp.exp(t) + s
        total = total + t
    exact[...] = state
    heads = key_cols // CUE_WIDTH
    last = out.shape[0] > DV + 8
    pack(out, state, total, against(asked[...], state)[:heads] if last else None)


def final_kernel(asked, mine, other, exact, cache_h, read_h, cache, read, sems, *, bit):
    heads, kept, _ = cache.shape
    key_cols = asked.shape[1]
    earlier = lax.bitwise_and(lax.axis_index("sp"), bit) == 0
    s_m, l_m, tail_m = unpack(mine, key_cols)
    s_o, l_o, tail_o = unpack(other, key_cols)
    fading = jnp.exp(jnp.where(earlier, l_o, l_m))
    first = jnp.where(earlier, s_m, s_o) * fading
    state = jnp.where(earlier, exact[...] * fading + s_o, first + exact[...])
    rows = heads * kept
    rows += -rows % 8
    row = lax.broadcasted_iota(jnp.int32, (rows, key_cols), 0)
    lane = lax.broadcasted_iota(jnp.int32, (rows, key_cols), 1)
    start = lax.axis_index("sp") * kept
    column = lax.div(row, kept) * CUE_WIDTH + start + lax.rem(row, kept)
    chosen = ((row < heads * kept) & (lane == column)).astype(F32)
    result = against(chosen, state)
    for h in range(heads):
        cache[h] = result[h * kept : (h + 1) * kept].astype(BF16)
    send = pltpu.make_async_copy(cache, cache_h, sems.at[0])
    send.start()
    heard = against(asked[...], first)[:heads]
    heard = heard + heard_of(jnp.where(earlier, tail_o, tail_m), heads)
    mean = jnp.mean(heard * heard, axis=-1, keepdims=True)
    read[...] = (heard * lax.rsqrt(mean + 1.0)).astype(BF16)
    last = pltpu.make_async_copy(read, read_h, sems.at[1])
    last.start()
    send.wait()
    last.wait()


VM = pl.BlockSpec(memory_space=pltpu.VMEM)


def call(kernel, out_shape, in_specs, scratch=(), flops=0, out_space=pltpu.VMEM):
    return pl.pallas_call(
        kernel,
        out_shape=out_shape,
        in_specs=in_specs,
        out_specs=jax.tree.map(lambda _: pl.BlockSpec(memory_space=out_space), out_shape),
        scratch_shapes=list(scratch),
        cost_estimate=pl.CostEstimate(flops=flops, bytes_accessed=0, transcendentals=0),
        compiler_params=pltpu.CompilerParams(vmem_limit_bytes=VMEM_LIMIT),
    )


def whole(sp, tp, tokens, wk, wv, wd, decay_offset, fresh_question):
    rows, width = tokens.shape
    key_cols, value_cols = wk.shape[1], wv.shape[1]
    heads = key_cols // CUE_WIDTH
    cols = 2 * key_cols + value_cols
    log_length = math.log(rows * tp * sp)
    offset = decay_offset.reshape(1, key_cols)
    sds = jax.ShapeDtypeStruct
    state_sds = sds((DV, key_cols), F32)
    total_sds = sds((1, key_cols), F32)

    edges = [rows * sum(ROW_PARTS[:n]) // sum(ROW_PARTS) for n in range(len(ROW_PARTS) + 1)]
    sides = [width * sum(COL_PARTS[:n]) // sum(COL_PARTS) for n in range(LATE + 1)]
    cuts = [(lo, hi, 0, width) for lo, hi in zip(edges[:-2], edges[1:-1])]
    cuts += [(edges[-2], edges[-1], lo, hi) for lo, hi in zip(sides[:-1], sides[1:])]
    held = pltpu.with_memory_space_constraint(tokens, pltpu.HBM)
    pieces = []
    for some in (cuts[:1], cuts[1:]):
        pieces += call(
            functools.partial(cut_kernel, cuts=tuple(some)),
            tuple(pltpu.VMEM((h - l, r - c), BF16) for l, h, c, r in some),
            [pl.BlockSpec(memory_space=pltpu.HBM)],
            [pltpu.SemaphoreType.DMA((len(some),))],
        )(held)
    far = {}
    for bit in range(1, tp // 2):
        for part, piece in enumerate(pieces):
            far[bit, part] = lax.ppermute(piece, "tp", swap(tp, 2 * bit))
    sibling = lax.ppermute(tokens, "tp", swap(tp, 1))

    hbm = pl.BlockSpec(memory_space=pltpu.HBM)
    weights = [pltpu.with_memory_space_constraint(w, pltpu.HBM) for w in (wk, wv, wd)]
    wk, wv, wd, s_near, l_near = call(
        functools.partial(near_kernel, log_length=log_length),
        tuple(pltpu.VMEM(w.shape, BF16) for w in weights) + (state_sds, total_sds),
        [VM, VM, hbm, hbm, hbm, VM],
        [pltpu.SemaphoreType.DMA((3,))],
        flops=4 * rows * width * cols,
    )(tokens, sibling, *weights, offset)

    asked = call(ask_kernel, sds((heads + -heads % 8, key_cols), F32), [VM])(fresh_question)

    blocks, states, totals = [None], [s_near], [l_near]
    pairs = {}
    for bit, part in far:
        pairs[bit, part] = (far[bit, part], lax.ppermute(far[bit, part], "tp", swap(tp, 1)))
    final_bit = tp // 2 - 1
    last = [pairs[final_bit, len(cuts) - LATE + n] for n in range(LATE)]
    for bit in range(1, tp // 2):
        taken = [pairs[bit, n] for n in range(len(cuts) - (LATE if bit == final_bit else 0))]
        inputs = [pair[side] for side in (0, 1) for pair in taken]
        far_rows = edges[-2] if bit == final_bit else rows
        s_a, s_b, l_a, l_b = call(
            functools.partial(
                early_kernel,
                log_length=log_length,
                pieces=len(taken),
                split=bit != final_bit,
            ),
            (state_sds, state_sds, total_sds, total_sds),
            [VM] * (len(inputs) + 4),
            flops=4 * far_rows * width * cols,
        )(*inputs, wk, wv, wd, offset)
        blocks += [(bit, 0, True), (bit, 0, False)]
        states += [s_a, s_b]
        totals += [l_a, l_b]
    late_rows = 2 * (edges[-1] - edges[-2])
    sums = call(
        partial_kernel,
        tuple(sds((late_rows, w.shape[1]), F32) for w in (wk, wv, wd)),
        [VM] * 5,
        flops=2 * late_rows * sides[1] * cols,
    )(*last[0], wk, wv, wd)
    payload = call(
        functools.partial(
            late_kernel, log_length=log_length, blocks=tuple(blocks), here=(final_bit, 1), parts=2
        ),
        payload_sds(heads, sp == 2),
        [VM] * (9 + 2 * len(blocks)),
        flops=2 * late_rows * (width - sides[1]) * cols,
    )(*last[1], *sums, wk, wv, wd, offset, *states, *totals)

    bits = [1 << n for n in range(sp.bit_length() - 1)]
    while len(bits) > 1:
        take = 2 if len(bits) > 2 else 1
        group, bits = bits[:take], bits[take:]
        others = []
        for k in range(1, 2**take):
            far_bits = sum(b for n, b in enumerate(group) if k >> n & 1)
            others.append(lax.ppermute(payload, "sp", swap(sp, far_bits)))
        payload, exact = call(
            functools.partial(merge_kernel, bits=tuple(group)),
            (payload_sds(heads, len(bits) == 1), state_sds),
            [VM] * (2 + len(others)),
        )(asked, payload, *others)
    other = lax.ppermute(payload, "sp", swap(sp, bits[0]))
    outs = (sds((heads, CUE_WIDTH // sp, DV), BF16), sds((heads, DV), BF16))
    return call(
        functools.partial(final_kernel, bit=bits[0]),
        outs,
        [VM] * 4,
        [pltpu.VMEM(o.shape, o.dtype) for o in outs] + [pltpu.SemaphoreType.DMA((2,))],
        out_space=pltpu.HBM,
    )(asked, payload, other, exact)


def solution(mesh):
    sp, tp = mesh.shape["sp"], mesh.shape["tp"]
    in_specs = (
        P(("sp", "tp"), None),
        P(None, "tp"),
        P(None, "tp"),
        P(None, "tp"),
        P("tp"),
        P("tp", None),
    )
    out_specs = (P("tp", "sp", None), P("tp", None))
    return jax.shard_map(
        functools.partial(whole, sp, tp),
        mesh=mesh,
        in_specs=in_specs,
        out_specs=out_specs,
        check_vma=False,
    )
```

```python
import functools
import math

import jax
import jax.numpy as jnp
from jax import lax
from jax.experimental import pallas as pl
from jax.experimental.pallas import tpu as pltpu
from jax.sharding import PartitionSpec as P


CUE_WIDTH = 64
DV = 128
DECAY_TAU = 16.0
ROW_PARTS = (2, 3, 3)
COL_PARTS = (8, 5, 3)
LATE = len(COL_PARTS)
VMEM_LIMIT = 8 * 1024 * 1024


F32 = jnp.float32
BF16 = jnp.bfloat16
EXACT = lax.Precision.HIGHEST


def swap(count, bit):
    return [(i, i ^ bit) for i in range(count)]


def products(x, weights, start=0):
    stop = start + x.shape[1]
    return [jnp.dot(x, w[start:stop, :], preferred_element_type=F32) for w in weights]


def project(sums, offset, log_length):
    keys, values, pre = sums
    z = pre + offset + log_length
    log_decay = (jnp.minimum(z, 0.0) - jnp.log1p(jnp.exp(-jnp.abs(z)))) / DECAY_TAU
    return keys.astype(BF16), values.astype(BF16), log_decay


def later_within(log_decay, sizes):
    rows = log_decay.shape[0]
    i = lax.broadcasted_iota(jnp.int32, (rows, rows), 0)
    j = lax.broadcasted_iota(jnp.int32, (rows, rows), 1)
    mask = j > i
    edge = 0
    for size in sizes[:-1]:
        edge += size
        mask = mask & ((i >= edge) == (j >= edge))
    parts = jnp.concatenate([p.astype(BF16) for p in split(log_decay)], axis=1)
    sums = jnp.dot(mask.astype(BF16), parts, preferred_element_type=F32)
    cols = log_decay.shape[1]
    return sums[:, :cols] + sums[:, cols : 2 * cols] + sums[:, 2 * cols :]


def weigh(keys, after):
    exact = keys.astype(F32) * jnp.exp(after)
    high = exact.astype(BF16)
    return high, (exact - high.astype(F32)).astype(BF16)


def outer(values, weighted):
    high, low = weighted
    heads = high.shape[1] // CUE_WIDTH
    group = min(2, heads)
    cols = group * CUE_WIDTH
    parts = []
    for g in range(heads // group):
        w = jnp.concatenate([p[:, g * cols : (g + 1) * cols] for p in (high, low)], axis=1)
        v = values[:, g * group * DV : (g + 1) * group * DV]
        full = lax.dot_general(v, w, (((0,), (0,)), ((), ())), preferred_element_type=F32)
        full = full[:, :cols] + full[:, cols:]
        kept = full[:DV]
        if group == 2:
            lane = lax.broadcasted_iota(jnp.int32, kept.shape, 1)
            kept = jnp.where(lane < CUE_WIDTH, kept, full[DV:])
        parts.append(kept)
    return parts[0] if len(parts) == 1 else jnp.concatenate(parts, axis=1)


def payload_sds(heads, heard):
    rows = 3 + 3 * heads if heard else 3
    width = max(heads * CUE_WIDTH, DV)
    return jax.ShapeDtypeStruct((DV + rows + -rows % 8, width), BF16)


def split(exact):
    parts, rest = [], exact
    for _ in range(3):
        parts.append(rest.astype(BF16).astype(F32))
        rest = rest - parts[-1]
    return parts


def widen(x, width):
    extra = width - x.shape[1]
    return jnp.concatenate([x, jnp.zeros((x.shape[0], extra), x.dtype)], axis=1) if extra else x


def pack(out, state, total, heard=None):
    width = out.shape[1]
    rows = [widen(p, width) for p in split(total)]
    if heard is not None:
        for part in split(heard):
            part = widen(part, width)
            rows += [part[h : h + 1] for h in range(part.shape[0])]
    row = lax.broadcasted_iota(jnp.int32, (out.shape[0] - DV, width), 0)
    tail = jnp.zeros(row.shape, F32)
    for n, value in enumerate(rows):
        tail = jnp.where(row == n, value, tail)
    out[:DV, :] = widen(state.astype(BF16), width)
    out[DV:, :] = tail.astype(BF16)


def unpack(ref, key_cols):
    tail = ref[DV:, :].astype(F32)
    total = tail[0:1] + tail[1:2] + tail[2:3]
    return ref[:DV, :key_cols].astype(F32), total[:, :key_cols], tail


def heard_of(tail, heads):
    parts = [tail[3 + n * heads : 3 + (n + 1) * heads, :DV] for n in range(3)]
    return parts[0] + parts[1] + parts[2]


def ask_kernel(question, out):
    row = lax.broadcasted_iota(jnp.int32, out.shape, 0)
    lane = lax.broadcasted_iota(jnp.int32, out.shape, 1)
    heads = question.shape[0]
    asked = jnp.concatenate([question[...].astype(F32)] * heads, axis=1) * CUE_WIDTH ** (-0.5)
    if out.shape[0] > heads:
        spare = jnp.zeros((out.shape[0] - heads, out.shape[1]), F32)
        asked = jnp.concatenate([asked, spare], axis=0)
    out[...] = jnp.where(lax.div(lane, CUE_WIDTH) == row, asked, 0.0)


def against(left, state):
    return lax.dot_general(
        left, state, (((1,), (1,)), ((), ())), precision=EXACT, preferred_element_type=F32
    )


def cut_kernel(tokens, *refs, cuts):
    sems = refs[-1]
    copies = [
        pltpu.make_async_copy(tokens.at[lo:hi, left:right], out, sems.at[n])
        for n, ((lo, hi, left, right), out) in enumerate(zip(cuts, refs))
    ]
    for copy in copies:
        copy.start()
    for copy in copies:
        copy.wait()


def near_kernel(x0, x1, *refs, log_length):
    stored, off, kept, (s_out, l_out, sems) = refs[:3], refs[3], refs[4:7], refs[7:]
    loads = [pltpu.make_async_copy(h, v, sems.at[n]) for n, (h, v) in enumerate(zip(stored, kept))]
    for load in loads:
        load.start()
    core = lax.rem(lax.axis_index("tp"), 2)
    rows = x0.shape[0]
    x = jnp.concatenate([x0[...], x1[...]], axis=0)
    sums = []
    for load, w in zip(loads, kept):
        load.wait()
        sums += products(x, [w])
    keys, values, log_decay = project(sums, off[...], log_length)
    after = later_within(log_decay, [rows, rows])
    own = after[0:1] + log_decay[0:1]
    sib = after[rows : rows + 1] + log_decay[rows : rows + 1]
    own_tail = jnp.where(core == 0, sib, 0.0)
    sib_tail = jnp.where(core == 0, 0.0, own)
    row = lax.broadcasted_iota(jnp.int32, after.shape, 0)
    after = after + jnp.where(row < rows, own_tail, sib_tail)
    s_out[...] = outer(values, weigh(keys, after))
    l_out[...] = own + sib


def early_kernel(*refs, log_length, pieces, split):
    sides = []
    for side in (refs[:pieces], refs[pieces : 2 * pieces]):
        whole = [ref[...] for ref in side]
        if split:
            whole = whole[:-LATE] + [jnp.concatenate(whole[-LATE:], axis=1)]
        sides.append(jnp.concatenate(whole, axis=0))
    wk, wv, wd, off, s_a, s_b, l_a, l_b = refs[2 * pieces :]
    rows = sides[0].shape[0]
    x = jnp.concatenate(sides, axis=0)
    keys, values, log_decay = project(products(x, (wk, wv, wd)), off[...], log_length)
    after = later_within(log_decay, [rows, rows])
    weighted = weigh(keys, after)
    s_a[...] = outer(values[:rows], [w[:rows] for w in weighted])
    s_b[...] = outer(values[rows:], [w[rows:] for w in weighted])
    l_a[...] = after[0:1] + log_decay[0:1]
    l_b[...] = after[rows : rows + 1] + log_decay[rows : rows + 1]


def partial_kernel(xa, xb, wk, wv, wd, *refs, start):
    x = jnp.concatenate([xa[...], xb[...]], axis=0)
    outs = refs[-3:]
    for n, value in enumerate(products(x, (wk, wv, wd), start)):
        outs[n][...] = refs[n][...] + value if start else value


def late_kernel(xa, xb, ks, vs, ds, wk, wv, wd, off, *refs, log_length, blocks, here, parts):
    states = refs[: len(blocks)]
    totals = refs[len(blocks) : 2 * len(blocks)]
    out = refs[2 * len(blocks)]
    place = lax.axis_index("tp")
    core = lax.rem(place, 2)
    chip = lax.div(place, 2)
    rows = xa.shape[0]

    def position(block):
        if block is None:
            return chip * (2 * parts)
        bit, part, same = block
        parity = core if same else 1 - core
        return lax.bitwise_xor(chip, bit) * (2 * parts) + parity * parts + part

    x = jnp.concatenate([xa[...], xb[...]], axis=0)
    more = products(x, (wk, wv, wd), wk.shape[0] - x.shape[1])
    sums = [s[...] + m for s, m in zip((ks, vs, ds), more)]
    keys, values, log_decay = project(sums, off[...], log_length)
    after = later_within(log_decay, [rows, rows])
    own = [
        after[0:1] + log_decay[0:1],
        after[rows : rows + 1] + log_decay[rows : rows + 1],
    ]
    every = [(position(b), totals[n][...]) for n, b in enumerate(blocks)]
    mine = [position(here + (True,)), position(here + (False,))]
    every += list(zip(mine, own))

    def later_of(pos):
        acc = jnp.zeros_like(own[0])
        for p, t in every:
            acc = acc + jnp.where(p > pos, t, 0.0)
        return acc

    row = lax.broadcasted_iota(jnp.int32, after.shape, 0)
    after = after + jnp.where(row < rows, later_of(mine[0]), later_of(mine[1]))
    state = outer(values, weigh(keys, after))
    total = own[0] + own[1]
    for n in range(len(blocks)):
        pos, t = every[n]
        state = state + states[n][...] * jnp.exp(later_of(pos))
        total = total + t
    pack(out, state, total)


def merge_kernel(asked, *refs, bits):
    count = 2 ** len(bits)
    out, exact = refs[count:]
    key_cols = asked.shape[1]
    parts = [unpack(ref, key_cols)[:2] for ref in refs[:count]]
    for n, bit in enumerate(bits):
        turned = lax.bitwise_and(lax.axis_index("sp"), bit) != 0
        parts = [
            tuple(jnp.where(turned, x, y) for x, y in zip(parts[k ^ (1 << n)], parts[k]))
            for k in range(count)
        ]
    state, total = parts[0]
    for s, t in parts[1:]:
        state = state * jnp.exp(t) + s
        total = total + t
    exact[...] = state
    heads = key_cols // CUE_WIDTH
    last = out.shape[0] > DV + 8
    pack(out, state, total, against(asked[...], state)[:heads] if last else None)


def final_kernel(asked, mine, other, exact, cache_h, read_h, cache, read, sems, *, bit):
    heads, kept, _ = cache.shape
    key_cols = asked.shape[1]
    earlier = lax.bitwise_and(lax.axis_index("sp"), bit) == 0
    s_m, l_m, tail_m = unpack(mine, key_cols)
    s_o, l_o, tail_o = unpack(other, key_cols)
    fading = jnp.exp(jnp.where(earlier, l_o, l_m))
    first = jnp.where(earlier, s_m, s_o) * fading
    state = jnp.where(earlier, exact[...] * fading + s_o, first + exact[...])
    rows = heads * kept
    rows += -rows % 8
    row = lax.broadcasted_iota(jnp.int32, (rows, key_cols), 0)
    lane = lax.broadcasted_iota(jnp.int32, (rows, key_cols), 1)
    start = lax.axis_index("sp") * kept
    column = lax.div(row, kept) * CUE_WIDTH + start + lax.rem(row, kept)
    chosen = ((row < heads * kept) & (lane == column)).astype(F32)
    result = against(chosen, state)
    for h in range(heads):
        cache[h] = result[h * kept : (h + 1) * kept].astype(BF16)
    send = pltpu.make_async_copy(cache, cache_h, sems.at[0])
    send.start()
    heard = against(asked[...], first)[:heads]
    heard = heard + heard_of(jnp.where(earlier, tail_o, tail_m), heads)
    mean = jnp.mean(heard * heard, axis=-1, keepdims=True)
    read[...] = (heard * lax.rsqrt(mean + 1.0)).astype(BF16)
    last = pltpu.make_async_copy(read, read_h, sems.at[1])
    last.start()
    send.wait()
    last.wait()


VM = pl.BlockSpec(memory_space=pltpu.VMEM)


def call(kernel, out_shape, in_specs, scratch=(), flops=0, out_space=pltpu.VMEM):
    return pl.pallas_call(
        kernel,
        out_shape=out_shape,
        in_specs=in_specs,
        out_specs=jax.tree.map(lambda _: pl.BlockSpec(memory_space=out_space), out_shape),
        scratch_shapes=list(scratch),
        cost_estimate=pl.CostEstimate(flops=flops, bytes_accessed=0, transcendentals=0),
        compiler_params=pltpu.CompilerParams(vmem_limit_bytes=VMEM_LIMIT),
    )


def whole(sp, tp, tokens, wk, wv, wd, decay_offset, fresh_question):
    rows, width = tokens.shape
    key_cols, value_cols = wk.shape[1], wv.shape[1]
    heads = key_cols // CUE_WIDTH
    cols = 2 * key_cols + value_cols
    log_length = math.log(rows * tp * sp)
    offset = decay_offset.reshape(1, key_cols)
    sds = jax.ShapeDtypeStruct
    state_sds = sds((DV, key_cols), F32)
    total_sds = sds((1, key_cols), F32)

    edges = [rows * sum(ROW_PARTS[:n]) // sum(ROW_PARTS) for n in range(len(ROW_PARTS) + 1)]
    sides = [width * sum(COL_PARTS[:n]) // sum(COL_PARTS) for n in range(LATE + 1)]
    cuts = [(lo, hi, 0, width) for lo, hi in zip(edges[:-2], edges[1:-1])]
    cuts += [(edges[-2], edges[-1], lo, hi) for lo, hi in zip(sides[:-1], sides[1:])]
    held = pltpu.with_memory_space_constraint(tokens, pltpu.HBM)
    pieces = []
    for some in (cuts[:1], cuts[1:]):
        pieces += call(
            functools.partial(cut_kernel, cuts=tuple(some)),
            tuple(pltpu.VMEM((h - l, r - c), BF16) for l, h, c, r in some),
            [pl.BlockSpec(memory_space=pltpu.HBM)],
            [pltpu.SemaphoreType.DMA((len(some),))],
        )(held)
    far = {}
    for bit in range(1, tp // 2):
        for part, piece in enumerate(pieces):
            far[bit, part] = lax.ppermute(piece, "tp", swap(tp, 2 * bit))
    sibling = lax.ppermute(tokens, "tp", swap(tp, 1))

    hbm = pl.BlockSpec(memory_space=pltpu.HBM)
    weights = [pltpu.with_memory_space_constraint(w, pltpu.HBM) for w in (wk, wv, wd)]
    wk, wv, wd, s_near, l_near = call(
        functools.partial(near_kernel, log_length=log_length),
        tuple(pltpu.VMEM(w.shape, BF16) for w in weights) + (state_sds, total_sds),
        [VM, VM, hbm, hbm, hbm, VM],
        [pltpu.SemaphoreType.DMA((3,))],
        flops=4 * rows * width * cols,
    )(tokens, sibling, *weights, offset)

    asked = call(ask_kernel, sds((heads + -heads % 8, key_cols), F32), [VM])(fresh_question)

    blocks, states, totals = [None], [s_near], [l_near]
    pairs = {}
    for bit, part in far:
        pairs[bit, part] = (far[bit, part], lax.ppermute(far[bit, part], "tp", swap(tp, 1)))
    final_bit = tp // 2 - 1
    last = [pairs[final_bit, len(cuts) - LATE + n] for n in range(LATE)]
    for bit in range(1, tp // 2):
        taken = [pairs[bit, n] for n in range(len(cuts) - (LATE if bit == final_bit else 0))]
        inputs = [pair[side] for side in (0, 1) for pair in taken]
        far_rows = edges[-2] if bit == final_bit else rows
        s_a, s_b, l_a, l_b = call(
            functools.partial(
                early_kernel,
                log_length=log_length,
                pieces=len(taken),
                split=bit != final_bit,
            ),
            (state_sds, state_sds, total_sds, total_sds),
            [VM] * (len(inputs) + 4),
            flops=4 * far_rows * width * cols,
        )(*inputs, wk, wv, wd, offset)
        blocks += [(bit, 0, True), (bit, 0, False)]
        states += [s_a, s_b]
        totals += [l_a, l_b]
    late_rows = 2 * (edges[-1] - edges[-2])
    sums = []
    for n in range(LATE - 1):
        sums = call(
            functools.partial(partial_kernel, start=sides[n]),
            tuple(sds((late_rows, w.shape[1]), F32) for w in (wk, wv, wd)),
            [VM] * (5 + len(sums)),
            flops=2 * late_rows * (sides[n + 1] - sides[n]) * cols,
        )(*last[n], wk, wv, wd, *sums)
    payload = call(
        functools.partial(
            late_kernel, log_length=log_length, blocks=tuple(blocks), here=(final_bit, 1), parts=2
        ),
        payload_sds(heads, sp == 2),
        [VM] * (9 + 2 * len(blocks)),
        flops=2 * late_rows * (width - sides[-2]) * cols,
    )(*last[-1], *sums, wk, wv, wd, offset, *states, *totals)

    bits = [1 << n for n in range(sp.bit_length() - 1)]
    while len(bits) > 1:
        take = 2 if len(bits) > 2 else 1
        group, bits = bits[:take], bits[take:]
        others = []
        for k in range(1, 2**take):
            far_bits = sum(b for n, b in enumerate(group) if k >> n & 1)
            others.append(lax.ppermute(payload, "sp", swap(sp, far_bits)))
        payload, exact = call(
            functools.partial(merge_kernel, bits=tuple(group)),
            (payload_sds(heads, len(bits) == 1), state_sds),
            [VM] * (2 + len(others)),
        )(asked, payload, *others)
    other = lax.ppermute(payload, "sp", swap(sp, bits[0]))
    outs = (sds((heads, CUE_WIDTH // sp, DV), BF16), sds((heads, DV), BF16))
    return call(
        functools.partial(final_kernel, bit=bits[0]),
        outs,
        [VM] * 4,
        [pltpu.VMEM(o.shape, o.dtype) for o in outs] + [pltpu.SemaphoreType.DMA((2,))],
        out_space=pltpu.HBM,
    )(asked, payload, other, exact)


def solution(mesh):
    sp, tp = mesh.shape["sp"], mesh.shape["tp"]
    in_specs = (
        P(("sp", "tp"), None),
        P(None, "tp"),
        P(None, "tp"),
        P(None, "tp"),
        P("tp"),
        P("tp", None),
    )
    out_specs = (P("tp", "sp", None), P("tp", None))
    return jax.shard_map(
        functools.partial(whole, sp, tp),
        mesh=mesh,
        in_specs=in_specs,
        out_specs=out_specs,
        check_vma=False,
    )
```

```python
import functools
import math

import jax
import jax.numpy as jnp
from jax import lax
from jax.experimental import pallas as pl
from jax.experimental.pallas import tpu as pltpu
from jax.sharding import PartitionSpec as P


CUE_WIDTH = 64
DV = 128
DECAY_TAU = 16.0
ROW_PARTS = (2, 3, 3)
COL_PARTS = (16, 10, 3, 3)
LATE = len(COL_PARTS)
VMEM_LIMIT = 8 * 1024 * 1024


F32 = jnp.float32
BF16 = jnp.bfloat16


def swap(count, bit):
    return [(i, i ^ bit) for i in range(count)]


def products(x, weights, start=0):
    stop = start + x.shape[1]
    return [jnp.dot(x, w[start:stop, :], preferred_element_type=F32) for w in weights]


def project(sums, offset, log_length):
    keys, values, pre = sums
    z = pre + offset + log_length
    log_decay = (jnp.minimum(z, 0.0) - jnp.log1p(jnp.exp(-jnp.abs(z)))) / DECAY_TAU
    return keys.astype(BF16), values.astype(BF16), log_decay


def later_within(log_decay, sizes):
    rows = log_decay.shape[0]
    i = lax.broadcasted_iota(jnp.int32, (rows, rows), 0)
    j = lax.broadcasted_iota(jnp.int32, (rows, rows), 1)
    mask = j > i
    edge = 0
    for size in sizes[:-1]:
        edge += size
        mask = mask & ((i >= edge) == (j >= edge))
    parts = jnp.concatenate([p.astype(BF16) for p in split(log_decay)], axis=1)
    sums = jnp.dot(mask.astype(BF16), parts, preferred_element_type=F32)
    cols = log_decay.shape[1]
    return sums[:, :cols] + sums[:, cols : 2 * cols] + sums[:, 2 * cols :]


def weigh(keys, after):
    exact = keys.astype(F32) * jnp.exp(after)
    high = exact.astype(BF16)
    return high, (exact - high.astype(F32)).astype(BF16)


def outer(values, weighted):
    high, low = weighted
    heads = high.shape[1] // CUE_WIDTH
    group = min(2, heads)
    cols = group * CUE_WIDTH
    parts = []
    for g in range(heads // group):
        w = jnp.concatenate([p[:, g * cols : (g + 1) * cols] for p in (high, low)], axis=1)
        v = values[:, g * group * DV : (g + 1) * group * DV]
        full = lax.dot_general(v, w, (((0,), (0,)), ((), ())), preferred_element_type=F32)
        full = full[:, :cols] + full[:, cols:]
        kept = full[:DV]
        if group == 2:
            lane = lax.broadcasted_iota(jnp.int32, kept.shape, 1)
            kept = jnp.where(lane < CUE_WIDTH, kept, full[DV:])
        parts.append(kept)
    return parts[0] if len(parts) == 1 else jnp.concatenate(parts, axis=1)


def payload_sds(heads, heard):
    rows = 3 + 3 * heads if heard else 3
    width = max(heads * CUE_WIDTH, DV)
    return jax.ShapeDtypeStruct((DV + rows + -rows % 8, width), BF16)


def split(exact):
    parts, rest = [], exact
    for _ in range(3):
        parts.append(rest.astype(BF16).astype(F32))
        rest = rest - parts[-1]
    return parts


def widen(x, width):
    extra = width - x.shape[1]
    return jnp.concatenate([x, jnp.zeros((x.shape[0], extra), x.dtype)], axis=1) if extra else x


def pack(out, state, total, heard=None):
    width = out.shape[1]
    rows = [widen(p, width) for p in split(total)]
    if heard is not None:
        for part in split(heard):
            part = widen(part, width)
            rows += [part[h : h + 1] for h in range(part.shape[0])]
    row = lax.broadcasted_iota(jnp.int32, (out.shape[0] - DV, width), 0)
    tail = jnp.zeros(row.shape, F32)
    for n, value in enumerate(rows):
        tail = jnp.where(row == n, value, tail)
    out[:DV, :] = widen(state.astype(BF16), width)
    out[DV:, :] = tail.astype(BF16)


def unpack(ref, key_cols):
    tail = ref[DV:, :].astype(F32)
    total = tail[0:1] + tail[1:2] + tail[2:3]
    return ref[:DV, :key_cols].astype(F32), total[:, :key_cols], tail


def heard_of(tail, heads):
    parts = [tail[3 + n * heads : 3 + (n + 1) * heads, :DV] for n in range(3)]
    return parts[0] + parts[1] + parts[2]


def ask_kernel(question, out):
    row = lax.broadcasted_iota(jnp.int32, out.shape, 0)
    lane = lax.broadcasted_iota(jnp.int32, out.shape, 1)
    heads = question.shape[0]
    asked = jnp.concatenate([question[...].astype(F32)] * heads, axis=1) * CUE_WIDTH ** (-0.5)
    if out.shape[0] > heads:
        spare = jnp.zeros((out.shape[0] - heads, out.shape[1]), F32)
        asked = jnp.concatenate([asked, spare], axis=0)
    out[...] = jnp.where(lax.div(lane, CUE_WIDTH) == row, asked, 0.0)


def against(left, state):
    left = left.astype(BF16)
    dims = (((1,), (1,)), ((), ()))
    high, mid, low = [
        lax.dot_general(left, p.astype(BF16), dims, preferred_element_type=F32)
        for p in split(state)
    ]
    return high + (mid + low)


def cut_kernel(tokens, *refs, cuts):
    sems = refs[-1]
    copies = [
        pltpu.make_async_copy(tokens.at[lo:hi, left:right], out, sems.at[n])
        for n, ((lo, hi, left, right), out) in enumerate(zip(cuts, refs))
    ]
    for copy in copies:
        copy.start()
    for copy in copies:
        copy.wait()


def near_kernel(x0, x1, *refs, log_length):
    stored, off, kept, (s_out, l_out, sems) = refs[:3], refs[3], refs[4:7], refs[7:]
    loads = [pltpu.make_async_copy(h, v, sems.at[n]) for n, (h, v) in enumerate(zip(stored, kept))]
    for load in loads:
        load.start()
    core = lax.rem(lax.axis_index("tp"), 2)
    rows = x0.shape[0]
    x = jnp.concatenate([x0[...], x1[...]], axis=0)
    sums = []
    for load, w in zip(loads, kept):
        load.wait()
        sums += products(x, [w])
    keys, values, log_decay = project(sums, off[...], log_length)
    after = later_within(log_decay, [rows, rows])
    own = after[0:1] + log_decay[0:1]
    sib = after[rows : rows + 1] + log_decay[rows : rows + 1]
    own_tail = jnp.where(core == 0, sib, 0.0)
    sib_tail = jnp.where(core == 0, 0.0, own)
    row = lax.broadcasted_iota(jnp.int32, after.shape, 0)
    after = after + jnp.where(row < rows, own_tail, sib_tail)
    s_out[...] = outer(values, weigh(keys, after))
    l_out[...] = own + sib


def early_kernel(*refs, log_length, pieces, split):
    sides = []
    for side in (refs[:pieces], refs[pieces : 2 * pieces]):
        whole = [ref[...] for ref in side]
        if split:
            whole = whole[:-LATE] + [jnp.concatenate(whole[-LATE:], axis=1)]
        sides.append(jnp.concatenate(whole, axis=0))
    wk, wv, wd, off, s_a, s_b, l_a, l_b = refs[2 * pieces :]
    rows = sides[0].shape[0]
    x = jnp.concatenate(sides, axis=0)
    keys, values, log_decay = project(products(x, (wk, wv, wd)), off[...], log_length)
    after = later_within(log_decay, [rows, rows])
    weighted = weigh(keys, after)
    s_a[...] = outer(values[:rows], [w[:rows] for w in weighted])
    s_b[...] = outer(values[rows:], [w[rows:] for w in weighted])
    l_a[...] = after[0:1] + log_decay[0:1]
    l_b[...] = after[rows : rows + 1] + log_decay[rows : rows + 1]


def partial_kernel(xa, xb, wk, wv, wd, *refs, start):
    x = jnp.concatenate([xa[...], xb[...]], axis=0)
    outs = refs[-3:]
    for n, value in enumerate(products(x, (wk, wv, wd), start)):
        outs[n][...] = refs[n][...] + value if start else value


def late_kernel(xa, xb, ks, vs, ds, wk, wv, wd, off, *refs, log_length, blocks, here, parts):
    states = refs[: len(blocks)]
    totals = refs[len(blocks) : 2 * len(blocks)]
    out = refs[2 * len(blocks)]
    place = lax.axis_index("tp")
    core = lax.rem(place, 2)
    chip = lax.div(place, 2)
    rows = xa.shape[0]

    def position(block):
        if block is None:
            return chip * (2 * parts)
        bit, part, same = block
        parity = core if same else 1 - core
        return lax.bitwise_xor(chip, bit) * (2 * parts) + parity * parts + part

    x = jnp.concatenate([xa[...], xb[...]], axis=0)
    more = products(x, (wk, wv, wd), wk.shape[0] - x.shape[1])
    sums = [s[...] + m for s, m in zip((ks, vs, ds), more)]
    keys, values, log_decay = project(sums, off[...], log_length)
    after = later_within(log_decay, [rows, rows])
    own = [
        after[0:1] + log_decay[0:1],
        after[rows : rows + 1] + log_decay[rows : rows + 1],
    ]
    every = [(position(b), totals[n][...]) for n, b in enumerate(blocks)]
    mine = [position(here + (True,)), position(here + (False,))]
    every += list(zip(mine, own))

    def later_of(pos):
        acc = jnp.zeros_like(own[0])
        for p, t in every:
            acc = acc + jnp.where(p > pos, t, 0.0)
        return acc

    row = lax.broadcasted_iota(jnp.int32, after.shape, 0)
    after = after + jnp.where(row < rows, later_of(mine[0]), later_of(mine[1]))
    state = outer(values, weigh(keys, after))
    total = own[0] + own[1]
    for n in range(len(blocks)):
        pos, t = every[n]
        state = state + states[n][...] * jnp.exp(later_of(pos))
        total = total + t
    pack(out, state, total)


def merge_kernel(asked, *refs, bits):
    count = 2 ** len(bits)
    out, exact = refs[count:]
    key_cols = asked.shape[1]
    parts = [unpack(ref, key_cols)[:2] for ref in refs[:count]]
    for n, bit in enumerate(bits):
        turned = lax.bitwise_and(lax.axis_index("sp"), bit) != 0
        parts = [
            tuple(jnp.where(turned, x, y) for x, y in zip(parts[k ^ (1 << n)], parts[k]))
            for k in range(count)
        ]
    state, total = parts[0]
    for s, t in parts[1:]:
        state = state * jnp.exp(t) + s
        total = total + t
    exact[...] = state
    heads = key_cols // CUE_WIDTH
    last = out.shape[0] > DV + 8
    pack(out, state, total, against(asked[...], state)[:heads] if last else None)


def final_kernel(asked, mine, other, exact, cache_h, read_h, cache, read, sems, *, bit):
    heads, kept, _ = cache.shape
    key_cols = asked.shape[1]
    earlier = lax.bitwise_and(lax.axis_index("sp"), bit) == 0
    s_m, l_m, tail_m = unpack(mine, key_cols)
    s_o, l_o, tail_o = unpack(other, key_cols)
    fading = jnp.exp(jnp.where(earlier, l_o, l_m))
    first = jnp.where(earlier, s_m, s_o) * fading
    state = jnp.where(earlier, exact[...] * fading + s_o, first + exact[...])
    rows = heads * kept
    rows += -rows % 8
    row = lax.broadcasted_iota(jnp.int32, (rows, key_cols), 0)
    lane = lax.broadcasted_iota(jnp.int32, (rows, key_cols), 1)
    start = lax.axis_index("sp") * kept
    column = lax.div(row, kept) * CUE_WIDTH + start + lax.rem(row, kept)
    chosen = ((row < heads * kept) & (lane == column)).astype(F32)
    result = against(chosen, state)
    for h in range(heads):
        cache[h] = result[h * kept : (h + 1) * kept].astype(BF16)
    send = pltpu.make_async_copy(cache, cache_h, sems.at[0])
    send.start()
    heard = against(asked[...], first)[:heads]
    heard = heard + heard_of(jnp.where(earlier, tail_o, tail_m), heads)
    mean = jnp.mean(heard * heard, axis=-1, keepdims=True)
    read[...] = (heard * lax.rsqrt(mean + 1.0)).astype(BF16)
    last = pltpu.make_async_copy(read, read_h, sems.at[1])
    last.start()
    send.wait()
    last.wait()


VM = pl.BlockSpec(memory_space=pltpu.VMEM)


def call(kernel, out_shape, in_specs, scratch=(), flops=0, out_space=pltpu.VMEM):
    return pl.pallas_call(
        kernel,
        out_shape=out_shape,
        in_specs=in_specs,
        out_specs=jax.tree.map(lambda _: pl.BlockSpec(memory_space=out_space), out_shape),
        scratch_shapes=list(scratch),
        cost_estimate=pl.CostEstimate(flops=flops, bytes_accessed=0, transcendentals=0),
        compiler_params=pltpu.CompilerParams(vmem_limit_bytes=VMEM_LIMIT),
    )


def whole(sp, tp, tokens, wk, wv, wd, decay_offset, fresh_question):
    rows, width = tokens.shape
    key_cols, value_cols = wk.shape[1], wv.shape[1]
    heads = key_cols // CUE_WIDTH
    cols = 2 * key_cols + value_cols
    log_length = math.log(rows * tp * sp)
    offset = decay_offset.reshape(1, key_cols)
    sds = jax.ShapeDtypeStruct
    state_sds = sds((DV, key_cols), F32)
    total_sds = sds((1, key_cols), F32)

    edges = [rows * sum(ROW_PARTS[:n]) // sum(ROW_PARTS) for n in range(len(ROW_PARTS) + 1)]
    sides = [width * sum(COL_PARTS[:n]) // sum(COL_PARTS) for n in range(LATE + 1)]
    cuts = [(lo, hi, 0, width) for lo, hi in zip(edges[:-2], edges[1:-1])]
    cuts += [(edges[-2], edges[-1], lo, hi) for lo, hi in zip(sides[:-1], sides[1:])]
    held = pltpu.with_memory_space_constraint(tokens, pltpu.HBM)
    pieces = []
    for some in (cuts[:1], cuts[1:]):
        pieces += call(
            functools.partial(cut_kernel, cuts=tuple(some)),
            tuple(pltpu.VMEM((h - l, r - c), BF16) for l, h, c, r in some),
            [pl.BlockSpec(memory_space=pltpu.HBM)],
            [pltpu.SemaphoreType.DMA((len(some),))],
        )(held)
    far = {}
    for bit in range(1, tp // 2):
        for part, piece in enumerate(pieces):
            far[bit, part] = lax.ppermute(piece, "tp", swap(tp, 2 * bit))
    sibling = lax.ppermute(tokens, "tp", swap(tp, 1))

    hbm = pl.BlockSpec(memory_space=pltpu.HBM)
    weights = [pltpu.with_memory_space_constraint(w, pltpu.HBM) for w in (wk, wv, wd)]
    wk, wv, wd, s_near, l_near = call(
        functools.partial(near_kernel, log_length=log_length),
        tuple(pltpu.VMEM(w.shape, BF16) for w in weights) + (state_sds, total_sds),
        [VM, VM, hbm, hbm, hbm, VM],
        [pltpu.SemaphoreType.DMA((3,))],
        flops=4 * rows * width * cols,
    )(tokens, sibling, *weights, offset)

    asked = call(ask_kernel, sds((heads + -heads % 8, key_cols), F32), [VM])(fresh_question)

    blocks, states, totals = [None], [s_near], [l_near]
    pairs = {}
    for bit, part in far:
        if part == len(pieces) - 1:
            other = lax.ppermute(pieces[part], "tp", swap(tp, 2 * bit + 1))
        else:
            other = lax.ppermute(far[bit, part], "tp", swap(tp, 1))
        pairs[bit, part] = (far[bit, part], other)
    final_bit = tp // 2 - 1
    last = [pairs[final_bit, len(cuts) - LATE + n] for n in range(LATE)]
    for bit in range(1, tp // 2):
        taken = [pairs[bit, n] for n in range(len(cuts) - (LATE if bit == final_bit else 0))]
        inputs = [pair[side] for side in (0, 1) for pair in taken]
        far_rows = edges[-2] if bit == final_bit else rows
        s_a, s_b, l_a, l_b = call(
            functools.partial(
                early_kernel,
                log_length=log_length,
                pieces=len(taken),
                split=bit != final_bit,
            ),
            (state_sds, state_sds, total_sds, total_sds),
            [VM] * (len(inputs) + 4),
            flops=4 * far_rows * width * cols,
        )(*inputs, wk, wv, wd, offset)
        blocks += [(bit, 0, True), (bit, 0, False)]
        states += [s_a, s_b]
        totals += [l_a, l_b]
    late_rows = 2 * (edges[-1] - edges[-2])
    sums = []
    for n in range(LATE - 1):
        sums = call(
            functools.partial(partial_kernel, start=sides[n]),
            tuple(sds((late_rows, w.shape[1]), F32) for w in (wk, wv, wd)),
            [VM] * (5 + len(sums)),
            flops=2 * late_rows * (sides[n + 1] - sides[n]) * cols,
        )(*last[n], wk, wv, wd, *sums)
    payload = call(
        functools.partial(
            late_kernel, log_length=log_length, blocks=tuple(blocks), here=(final_bit, 1), parts=2
        ),
        payload_sds(heads, sp == 2),
        [VM] * (9 + 2 * len(blocks)),
        flops=2 * late_rows * (width - sides[-2]) * cols,
    )(*last[-1], *sums, wk, wv, wd, offset, *states, *totals)

    bits = [1 << n for n in range(sp.bit_length() - 1)]
    while len(bits) > 1:
        take = 2 if len(bits) > 2 else 1
        group, bits = bits[:take], bits[take:]
        others = []
        for k in range(1, 2**take):
            far_bits = sum(b for n, b in enumerate(group) if k >> n & 1)
            others.append(lax.ppermute(payload, "sp", swap(sp, far_bits)))
        payload, exact = call(
            functools.partial(merge_kernel, bits=tuple(group)),
            (payload_sds(heads, len(bits) == 1), state_sds),
            [VM] * (2 + len(others)),
        )(asked, payload, *others)
    other = lax.ppermute(payload, "sp", swap(sp, bits[0]))
    outs = (sds((heads, CUE_WIDTH // sp, DV), BF16), sds((heads, DV), BF16))
    return call(
        functools.partial(final_kernel, bit=bits[0]),
        outs,
        [VM] * 4,
        [pltpu.VMEM(o.shape, o.dtype) for o in outs] + [pltpu.SemaphoreType.DMA((2,))],
        out_space=pltpu.HBM,
    )(asked, payload, other, exact)


def solution(mesh):
    sp, tp = mesh.shape["sp"], mesh.shape["tp"]
    in_specs = (
        P(("sp", "tp"), None),
        P(None, "tp"),
        P(None, "tp"),
        P(None, "tp"),
        P("tp"),
        P("tp", None),
    )
    out_specs = (P("tp", "sp", None), P("tp", None))
    return jax.shard_map(
        functools.partial(whole, sp, tp),
        mesh=mesh,
        in_specs=in_specs,
        out_specs=out_specs,
        check_vma=False,
    )
```

```python
import functools
import math

import jax
import jax.numpy as jnp
from jax import lax
from jax.experimental import pallas as pl
from jax.experimental.pallas import tpu as pltpu
from jax.sharding import PartitionSpec as P


CUE_WIDTH = 64
DV = 128
DECAY_TAU = 16.0
ROW_PARTS = (2, 3, 3)
COL_PARTS = (8, 5, 3)
LATE = len(COL_PARTS)
VMEM_LIMIT = 8 * 1024 * 1024


F32 = jnp.float32
BF16 = jnp.bfloat16


def swap(count, bit):
    return [(i, i ^ bit) for i in range(count)]


def products(x, weights, start=0):
    stop = start + x.shape[1]
    return [jnp.dot(x, w[start:stop, :], preferred_element_type=F32) for w in weights]


def project(sums, offset, log_length):
    keys, values, pre = sums
    z = pre + offset + log_length
    log_decay = (jnp.minimum(z, 0.0) - jnp.log1p(jnp.exp(-jnp.abs(z)))) / DECAY_TAU
    return keys.astype(BF16), values.astype(BF16), log_decay


def later_within(log_decay, sizes):
    rows = log_decay.shape[0]
    i = lax.broadcasted_iota(jnp.int32, (rows, rows), 0)
    j = lax.broadcasted_iota(jnp.int32, (rows, rows), 1)
    mask = j > i
    edge = 0
    for size in sizes[:-1]:
        edge += size
        mask = mask & ((i >= edge) == (j >= edge))
    parts = jnp.concatenate([p.astype(BF16) for p in split(log_decay)], axis=1)
    sums = jnp.dot(mask.astype(BF16), parts, preferred_element_type=F32)
    cols = log_decay.shape[1]
    return sums[:, :cols] + sums[:, cols : 2 * cols] + sums[:, 2 * cols :]


def weigh(keys, after):
    exact = keys.astype(F32) * jnp.exp(after)
    high = exact.astype(BF16)
    return high, (exact - high.astype(F32)).astype(BF16)


def outer(values, weighted):
    high, low = weighted
    heads = high.shape[1] // CUE_WIDTH
    group = min(2, heads)
    cols = group * CUE_WIDTH
    parts = []
    for g in range(heads // group):
        w = jnp.concatenate([p[:, g * cols : (g + 1) * cols] for p in (high, low)], axis=1)
        v = values[:, g * group * DV : (g + 1) * group * DV]
        full = lax.dot_general(v, w, (((0,), (0,)), ((), ())), preferred_element_type=F32)
        full = full[:, :cols] + full[:, cols:]
        kept = full[:DV]
        if group == 2:
            lane = lax.broadcasted_iota(jnp.int32, kept.shape, 1)
            kept = jnp.where(lane < CUE_WIDTH, kept, full[DV:])
        parts.append(kept)
    return parts[0] if len(parts) == 1 else jnp.concatenate(parts, axis=1)


def payload_sds(heads, heard):
    rows = 3 + 3 * heads if heard else 3
    width = max(heads * CUE_WIDTH, DV)
    return jax.ShapeDtypeStruct((DV + rows + -rows % 8, width), BF16)


def split(exact):
    parts, rest = [], exact
    for _ in range(3):
        parts.append(rest.astype(BF16).astype(F32))
        rest = rest - parts[-1]
    return parts


def widen(x, width):
    extra = width - x.shape[1]
    return jnp.concatenate([x, jnp.zeros((x.shape[0], extra), x.dtype)], axis=1) if extra else x


def pack(out, state, total, heard=None):
    width = out.shape[1]
    rows = [widen(p, width) for p in split(total)]
    if heard is not None:
        for part in split(heard):
            part = widen(part, width)
            rows += [part[h : h + 1] for h in range(part.shape[0])]
    row = lax.broadcasted_iota(jnp.int32, (out.shape[0] - DV, width), 0)
    tail = jnp.zeros(row.shape, F32)
    for n, value in enumerate(rows):
        tail = jnp.where(row == n, value, tail)
    out[:DV, :] = widen(state.astype(BF16), width)
    out[DV:, :] = tail.astype(BF16)


def unpack(ref, key_cols):
    tail = ref[DV:, :].astype(F32)
    total = tail[0:1] + tail[1:2] + tail[2:3]
    return ref[:DV, :key_cols].astype(F32), total[:, :key_cols], tail


def heard_of(tail, heads):
    parts = [tail[3 + n * heads : 3 + (n + 1) * heads, :DV] for n in range(3)]
    return parts[0] + parts[1] + parts[2]


def ask_kernel(question, out):
    row = lax.broadcasted_iota(jnp.int32, out.shape, 0)
    lane = lax.broadcasted_iota(jnp.int32, out.shape, 1)
    heads = question.shape[0]
    asked = jnp.concatenate([question[...].astype(F32)] * heads, axis=1) * CUE_WIDTH ** (-0.5)
    if out.shape[0] > heads:
        spare = jnp.zeros((out.shape[0] - heads, out.shape[1]), F32)
        asked = jnp.concatenate([asked, spare], axis=0)
    out[...] = jnp.where(lax.div(lane, CUE_WIDTH) == row, asked, 0.0)


def against(left, state):
    left = left.astype(BF16)
    dims = (((1,), (1,)), ((), ()))
    high, mid, low = [
        lax.dot_general(left, p.astype(BF16), dims, preferred_element_type=F32)
        for p in split(state)
    ]
    return high + (mid + low)


def cut_kernel(tokens, *refs, cuts):
    sems = refs[-1]
    copies = [
        pltpu.make_async_copy(tokens.at[lo:hi, left:right], out, sems.at[n])
        for n, ((lo, hi, left, right), out) in enumerate(zip(cuts, refs))
    ]
    for copy in copies:
        copy.start()
    for copy in copies:
        copy.wait()


def near_kernel(x0, x1, *refs, log_length):
    stored, off, kept, (s_out, l_out, sems) = refs[:3], refs[3], refs[4:7], refs[7:]
    loads = [pltpu.make_async_copy(h, v, sems.at[n]) for n, (h, v) in enumerate(zip(stored, kept))]
    for load in loads:
        load.start()
    core = lax.rem(lax.axis_index("tp"), 2)
    rows = x0.shape[0]
    x = jnp.concatenate([x0[...], x1[...]], axis=0)
    sums = []
    for load, w in zip(loads, kept):
        load.wait()
        sums += products(x, [w])
    keys, values, log_decay = project(sums, off[...], log_length)
    after = later_within(log_decay, [rows, rows])
    own = after[0:1] + log_decay[0:1]
    sib = after[rows : rows + 1] + log_decay[rows : rows + 1]
    own_tail = jnp.where(core == 0, sib, 0.0)
    sib_tail = jnp.where(core == 0, 0.0, own)
    row = lax.broadcasted_iota(jnp.int32, after.shape, 0)
    after = after + jnp.where(row < rows, own_tail, sib_tail)
    s_out[...] = outer(values, weigh(keys, after))
    l_out[...] = own + sib


def early_kernel(*refs, log_length, pieces, split):
    sides = []
    for side in (refs[:pieces], refs[pieces : 2 * pieces]):
        whole = [ref[...] for ref in side]
        if split:
            whole = whole[:-LATE] + [jnp.concatenate(whole[-LATE:], axis=1)]
        sides.append(jnp.concatenate(whole, axis=0))
    wk, wv, wd, off, s_a, s_b, l_a, l_b = refs[2 * pieces :]
    rows = sides[0].shape[0]
    x = jnp.concatenate(sides, axis=0)
    keys, values, log_decay = project(products(x, (wk, wv, wd)), off[...], log_length)
    after = later_within(log_decay, [rows, rows])
    weighted = weigh(keys, after)
    s_a[...] = outer(values[:rows], [w[:rows] for w in weighted])
    s_b[...] = outer(values[rows:], [w[rows:] for w in weighted])
    l_a[...] = after[0:1] + log_decay[0:1]
    l_b[...] = after[rows : rows + 1] + log_decay[rows : rows + 1]


def partial_kernel(xa, xb, wk, wv, wd, *refs, start):
    x = jnp.concatenate([xa[...], xb[...]], axis=0)
    outs = refs[-3:]
    for n, value in enumerate(products(x, (wk, wv, wd), start)):
        outs[n][...] = refs[n][...] + value if start else value


def late_kernel(xa, xb, ks, vs, ds, wk, wv, wd, off, *refs, log_length, blocks, here, parts):
    states = refs[: len(blocks)]
    totals = refs[len(blocks) : 2 * len(blocks)]
    out = refs[2 * len(blocks)]
    place = lax.axis_index("tp")
    core = lax.rem(place, 2)
    chip = lax.div(place, 2)
    rows = xa.shape[0]

    def position(block):
        if block is None:
            return chip * (2 * parts)
        bit, part, same = block
        parity = core if same else 1 - core
        return lax.bitwise_xor(chip, bit) * (2 * parts) + parity * parts + part

    x = jnp.concatenate([xa[...], xb[...]], axis=0)
    more = products(x, (wk, wv, wd), wk.shape[0] - x.shape[1])
    sums = [s[...] + m for s, m in zip((ks, vs, ds), more)]
    keys, values, log_decay = project(sums, off[...], log_length)
    after = later_within(log_decay, [rows, rows])
    own = [
        after[0:1] + log_decay[0:1],
        after[rows : rows + 1] + log_decay[rows : rows + 1],
    ]
    every = [(position(b), totals[n][...]) for n, b in enumerate(blocks)]
    mine = [position(here + (True,)), position(here + (False,))]
    every += list(zip(mine, own))

    def later_of(pos):
        acc = jnp.zeros_like(own[0])
        for p, t in every:
            acc = acc + jnp.where(p > pos, t, 0.0)
        return acc

    row = lax.broadcasted_iota(jnp.int32, after.shape, 0)
    after = after + jnp.where(row < rows, later_of(mine[0]), later_of(mine[1]))
    state = outer(values, weigh(keys, after))
    total = own[0] + own[1]
    for n in range(len(blocks)):
        pos, t = every[n]
        state = state + states[n][...] * jnp.exp(later_of(pos))
        total = total + t
    pack(out, state, total)


def merge_kernel(asked, *refs, bits):
    count = 2 ** len(bits)
    out, exact = refs[count:]
    key_cols = asked.shape[1]
    parts = [unpack(ref, key_cols)[:2] for ref in refs[:count]]
    for n, bit in enumerate(bits):
        turned = lax.bitwise_and(lax.axis_index("sp"), bit) != 0
        parts = [
            tuple(jnp.where(turned, x, y) for x, y in zip(parts[k ^ (1 << n)], parts[k]))
            for k in range(count)
        ]
    state, total = parts[0]
    for s, t in parts[1:]:
        state = state * jnp.exp(t) + s
        total = total + t
    exact[...] = state
    heads = key_cols // CUE_WIDTH
    last = out.shape[0] > DV + 8
    pack(out, state, total, against(asked[...], state)[:heads] if last else None)


def final_kernel(asked, mine, other, exact, cache_h, read_h, cache, read, sems, *, bit):
    heads, kept, _ = cache.shape
    key_cols = asked.shape[1]
    earlier = lax.bitwise_and(lax.axis_index("sp"), bit) == 0
    s_m, l_m, tail_m = unpack(mine, key_cols)
    s_o, l_o, tail_o = unpack(other, key_cols)
    fading = jnp.exp(jnp.where(earlier, l_o, l_m))
    first = jnp.where(earlier, s_m, s_o) * fading
    state = jnp.where(earlier, exact[...] * fading + s_o, first + exact[...])
    rows = heads * kept
    rows += -rows % 8
    row = lax.broadcasted_iota(jnp.int32, (rows, key_cols), 0)
    lane = lax.broadcasted_iota(jnp.int32, (rows, key_cols), 1)
    start = lax.axis_index("sp") * kept
    column = lax.div(row, kept) * CUE_WIDTH + start + lax.rem(row, kept)
    chosen = ((row < heads * kept) & (lane == column)).astype(F32)
    result = against(chosen, state)
    for h in range(heads):
        cache[h] = result[h * kept : (h + 1) * kept].astype(BF16)
    send = pltpu.make_async_copy(cache, cache_h, sems.at[0])
    send.start()
    heard = against(asked[...], first)[:heads]
    heard = heard + heard_of(jnp.where(earlier, tail_o, tail_m), heads)
    mean = jnp.mean(heard * heard, axis=-1, keepdims=True)
    read[...] = (heard * lax.rsqrt(mean + 1.0)).astype(BF16)
    last = pltpu.make_async_copy(read, read_h, sems.at[1])
    last.start()
    send.wait()
    last.wait()


VM = pl.BlockSpec(memory_space=pltpu.VMEM)


def call(kernel, out_shape, in_specs, scratch=(), flops=0, out_space=pltpu.VMEM):
    return pl.pallas_call(
        kernel,
        out_shape=out_shape,
        in_specs=in_specs,
        out_specs=jax.tree.map(lambda _: pl.BlockSpec(memory_space=out_space), out_shape),
        scratch_shapes=list(scratch),
        cost_estimate=pl.CostEstimate(flops=flops, bytes_accessed=0, transcendentals=0),
        compiler_params=pltpu.CompilerParams(vmem_limit_bytes=VMEM_LIMIT),
    )


def whole(sp, tp, tokens, wk, wv, wd, decay_offset, fresh_question):
    rows, width = tokens.shape
    key_cols, value_cols = wk.shape[1], wv.shape[1]
    heads = key_cols // CUE_WIDTH
    cols = 2 * key_cols + value_cols
    log_length = math.log(rows * tp * sp)
    offset = decay_offset.reshape(1, key_cols)
    sds = jax.ShapeDtypeStruct
    state_sds = sds((DV, key_cols), F32)
    total_sds = sds((1, key_cols), F32)

    edges = [rows * sum(ROW_PARTS[:n]) // sum(ROW_PARTS) for n in range(len(ROW_PARTS) + 1)]
    sides = [width * sum(COL_PARTS[:n]) // sum(COL_PARTS) for n in range(LATE + 1)]
    cuts = [(lo, hi, 0, width) for lo, hi in zip(edges[:-2], edges[1:-1])]
    cuts += [(edges[-2], edges[-1], lo, hi) for lo, hi in zip(sides[:-1], sides[1:])]
    held = pltpu.with_memory_space_constraint(tokens, pltpu.HBM)
    pieces = []
    for some in (cuts[:1], cuts[1:]):
        pieces += call(
            functools.partial(cut_kernel, cuts=tuple(some)),
            tuple(pltpu.VMEM((h - l, r - c), BF16) for l, h, c, r in some),
            [pl.BlockSpec(memory_space=pltpu.HBM)],
            [pltpu.SemaphoreType.DMA((len(some),))],
        )(held)
    far = {}
    for bit in range(1, tp // 2):
        for part, piece in enumerate(pieces):
            far[bit, part] = lax.ppermute(piece, "tp", swap(tp, 2 * bit))
    sibling = lax.ppermute(tokens, "tp", swap(tp, 1))

    hbm = pl.BlockSpec(memory_space=pltpu.HBM)
    weights = [pltpu.with_memory_space_constraint(w, pltpu.HBM) for w in (wk, wv, wd)]
    wk, wv, wd, s_near, l_near = call(
        functools.partial(near_kernel, log_length=log_length),
        tuple(pltpu.VMEM(w.shape, BF16) for w in weights) + (state_sds, total_sds),
        [VM, VM, hbm, hbm, hbm, VM],
        [pltpu.SemaphoreType.DMA((3,))],
        flops=4 * rows * width * cols,
    )(tokens, sibling, *weights, offset)

    asked = call(ask_kernel, sds((heads + -heads % 8, key_cols), F32), [VM])(fresh_question)

    blocks, states, totals = [None], [s_near], [l_near]
    pairs = {}
    for bit, part in far:
        pairs[bit, part] = (far[bit, part], lax.ppermute(far[bit, part], "tp", swap(tp, 1)))
    final_bit = tp // 2 - 1
    last = [pairs[final_bit, len(cuts) - LATE + n] for n in range(LATE)]
    for bit in range(1, tp // 2):
        taken = [pairs[bit, n] for n in range(len(cuts) - (LATE if bit == final_bit else 0))]
        inputs = [pair[side] for side in (0, 1) for pair in taken]
        far_rows = edges[-2] if bit == final_bit else rows
        s_a, s_b, l_a, l_b = call(
            functools.partial(
                early_kernel,
                log_length=log_length,
                pieces=len(taken),
                split=bit != final_bit,
            ),
            (state_sds, state_sds, total_sds, total_sds),
            [VM] * (len(inputs) + 4),
            flops=4 * far_rows * width * cols,
        )(*inputs, wk, wv, wd, offset)
        blocks += [(bit, 0, True), (bit, 0, False)]
        states += [s_a, s_b]
        totals += [l_a, l_b]
    late_rows = 2 * (edges[-1] - edges[-2])
    sums = []
    for n in range(LATE - 1):
        sums = call(
            functools.partial(partial_kernel, start=sides[n]),
            tuple(sds((late_rows, w.shape[1]), F32) for w in (wk, wv, wd)),
            [VM] * (5 + len(sums)),
            flops=2 * late_rows * (sides[n + 1] - sides[n]) * cols,
        )(*last[n], wk, wv, wd, *sums)
    payload = call(
        functools.partial(
            late_kernel, log_length=log_length, blocks=tuple(blocks), here=(final_bit, 1), parts=2
        ),
        payload_sds(heads, sp == 2),
        [VM] * (9 + 2 * len(blocks)),
        flops=2 * late_rows * (width - sides[-2]) * cols,
    )(*last[-1], *sums, wk, wv, wd, offset, *states, *totals)

    bits = [1 << n for n in range(sp.bit_length() - 1)]
    while len(bits) > 1:
        take = 2 if len(bits) > 2 else 1
        group, bits = bits[:take], bits[take:]
        others = []
        for k in range(1, 2**take):
            far_bits = sum(b for n, b in enumerate(group) if k >> n & 1)
            others.append(lax.ppermute(payload, "sp", swap(sp, far_bits)))
        payload, exact = call(
            functools.partial(merge_kernel, bits=tuple(group)),
            (payload_sds(heads, len(bits) == 1), state_sds),
            [VM] * (2 + len(others)),
        )(asked, payload, *others)
    other = lax.ppermute(payload, "sp", swap(sp, bits[0]))
    outs = (sds((heads, CUE_WIDTH // sp, DV), BF16), sds((heads, DV), BF16))
    return call(
        functools.partial(final_kernel, bit=bits[0]),
        outs,
        [VM] * 4,
        [pltpu.VMEM(o.shape, o.dtype) for o in outs] + [pltpu.SemaphoreType.DMA((2,))],
        out_space=pltpu.HBM,
    )(asked, payload, other, exact)


def solution(mesh):
    sp, tp = mesh.shape["sp"], mesh.shape["tp"]
    in_specs = (
        P(("sp", "tp"), None),
        P(None, "tp"),
        P(None, "tp"),
        P(None, "tp"),
        P("tp"),
        P("tp", None),
    )
    out_specs = (P("tp", "sp", None), P("tp", None))
    return jax.shard_map(
        functools.partial(whole, sp, tp),
        mesh=mesh,
        in_specs=in_specs,
        out_specs=out_specs,
        check_vma=False,
    )
```
